256 devices in a mesh: fs: 16 (over y, x), tp: 16 (over z, core).
Axes of the slice: x: 4, y: 4, z: 8, core: 2. Of those that a mesh axis runs over, the one named last changes fastest.
Arguments:
- normed: bfloat16 [16384, 4096], P('fs'), may hold values from -6 to 6
- query_cotangent: bfloat16 [16384, 4096], P('fs', 'tp'), may hold values from -0.059814453 to 0.059814453
- attended: bfloat16 [16384, 4096], P('fs', 'tp'), may hold values from -6 to 6
- output_cotangent: bfloat16 [16384, 4096], P('fs'), may hold values from -0.059814453 to 0.059814453
- query_basis: bfloat16 [4096, 128], replicated, may hold values from -0.09375 to 0.09375
- output_basis: bfloat16 [4096, 128], replicated, may hold values from -0.09375 to 0.09375
- query_master: float32 [4096, 4096], P('fs', 'tp'), may hold values from -0.6 to 0.6
- output_master: float32 [4096, 4096], P('fs', 'tp'), may hold values from -0.6 to 0.6
- query_first: float32 [128, 4096], P('fs', 'tp'), may hold values from -3 to 3
- query_second: float32 [128, 4096], P('fs', 'tp'), may hold values from 0.1 to 1
- output_first: float32 [128, 4096], P('fs', 'tp'), may hold values from -3 to 3
- output_second: float32 [128, 4096], P('fs', 'tp'), may hold values from 0.1 to 1
Outputs:
- query_first_new: float32 [128, 4096], P('fs', 'tp')
- query_second_new: float32 [128, 4096], P('fs', 'tp')
- query_step: float32 [4096, 4096], P('fs', 'tp')
- query_new: float32 [4096, 4096], P('fs', 'tp')
- query_copy: bfloat16 [4096, 4096], P(None, 'tp')
- output_first_new: float32 [128, 4096], P('fs', 'tp')
- output_second_new: float32 [128, 4096], P('fs', 'tp')
- output_step: float32 [4096, 4096], P('fs', 'tp')
- output_new: float32 [4096, 4096], P('fs', 'tp')
- output_copy: bfloat16 [4096, 4096], P(None, 'tp')
The draws below stay inside these ranges and needn't reach their ends.
All inputs are finite; a program needn't handle non-finite values.
Results may differ from the reference program's by a relative error of at most 0.0065.
Values may be sent and summed in bfloat16 or wider, within the bound.
A program may use at most 128 MiB of HBM per device.

```python
import math
import jax
import jax.numpy as jnp
from jax import lax

D = 4096
RANK = 128
QW = 4096
TOKENS = 16384


def block_levels(stream_key, dims, shards, least, largest):
    loudness, own = 1.0, jax.random.fold_in(stream_key, 6)
    for axis_at, blocks in shards:
        heights = jnp.exp(jax.random.uniform(jax.random.fold_in(own, axis_at), (blocks,), jnp.float32, least / len(shards), largest / len(shards)))
        loudness = loudness * jnp.repeat(heights, dims[axis_at] // blocks).reshape([-1 if axis == axis_at else 1 for axis in range(len(dims))])
    return loudness


def bell_draw(key, dims, spread, most, cuts=(), kind=jnp.bfloat16):
    result = jax.random.normal(key, dims, jnp.float32) * spread
    if len(cuts) > 0:
        result = block_levels(key, dims, cuts, -0.22, 0.18) * result
    return jnp.clip(result, min=-most, max=most).astype(kind)


def setup_inputs(seed: int = 0) -> dict:
    key_list = jax.random.split(jax.random.key(seed), 13)
    return {
        "normed": bell_draw(key_list[0], (TOKENS, D), 1.0, 6.0, ((0, 16),)),
        "query_cotangent": bell_draw(key_list[1], (TOKENS, QW), 0.01, 0.059814453, ((0, 16), (1, 16))),
        "attended": bell_draw(key_list[2], (TOKENS, QW), 1.0, 6.0, ((0, 16), (1, 16))),
        "output_cotangent": bell_draw(key_list[3], (TOKENS, D), 0.01, 0.059814453, ((0, 16),)),
        "query_basis": bell_draw(key_list[4], (D, RANK), D ** -0.5, 0.09375),
        "output_basis": bell_draw(key_list[5], (D, RANK), D ** -0.5, 0.09375),
        "query_master": bell_draw(key_list[6], (D, QW), 0.1, 0.6, ((0, 16), (1, 16)), jnp.float32),
        "output_master": bell_draw(key_list[7], (D, QW), 0.1, 0.6, ((0, 16), (1, 16)), jnp.float32),
        "query_first": bell_draw(key_list[8], (RANK, QW), 0.5, 3.0, ((0, 16), (1, 16)), jnp.float32),
        "query_second": jnp.clip(jnp.exp(math.log(1.0) - 2.3025851 * jax.random.uniform(key_list[9], (RANK, QW), jnp.float32) ** block_levels(key_list[9], (RANK, QW), ((0, 16), (1, 16)), -0.2, 0.2)), 0.1, 1.0),
        "output_first": bell_draw(key_list[10], (RANK, QW), 0.5, 3.0, ((0, 16), (1, 16)), jnp.float32),
        "output_second": jnp.clip(jnp.exp(math.log(1.0) - 2.3025851 * jax.random.uniform(key_list[11], (RANK, QW), jnp.float32) ** block_levels(key_list[11], (RANK, QW), ((0, 16), (1, 16)), -0.2, 0.2)), 0.1, 1.0),
    }


FIRST_DECAY = 0.7
SECOND_DECAY = 0.8
SECOND_FLOOR = 0.05
SCALE_FLOOR = 0.01
LEARN_RATE = 0.05

def adjust(gradient, basis, master, first, second):
    wide_basis = basis.astype(jnp.float32)
    lowered = jnp.dot(wide_basis.T, gradient, precision=lax.Precision.HIGHEST)
    first_new = FIRST_DECAY * first + (1.0 - FIRST_DECAY) * lowered
    second_new = SECOND_DECAY * second + (1.0 - SECOND_DECAY) * lowered * lowered
    ratios = first_new / jnp.sqrt(second_new + SECOND_FLOOR)
    update = jnp.dot(wide_basis, ratios, precision=lax.Precision.HIGHEST)
    factor = lax.rsqrt(jnp.mean(update * update) + SCALE_FLOOR)
    update_step = update * factor
    master_new = master - LEARN_RATE * update_step
    return (first_new, second_new, update_step, master_new, master_new.astype(jnp.bfloat16))

def reference(normed, query_cotangent, attended, output_cotangent, query_basis, output_basis, query_master, output_master, query_first, query_second, output_first, output_second):
    grad_query = jnp.dot(normed.T, query_cotangent, preferred_element_type=jnp.float32)
    grad_output = jnp.dot(output_cotangent.T, attended, preferred_element_type=jnp.float32)
    query_parts = adjust(grad_query, query_basis, query_master, query_first, query_second)
    output_parts = adjust(grad_output, output_basis, output_master, output_first, output_second)
    return (query_parts[0], query_parts[1], query_parts[2], query_parts[3], query_parts[4], output_parts[0], output_parts[1], output_parts[2], output_parts[3], output_parts[4])
```

```python
import jax
import jax.numpy as jnp
from jax import lax
from jax.experimental import pallas as pl
from jax.experimental.pallas import tpu as pltpu
from jax.sharding import PartitionSpec as P

FIRST_DECAY = 0.7
SECOND_DECAY = 0.8
SECOND_FLOOR = 0.05
SCALE_FLOOR = 0.01
LEARN_RATE = 0.05
OVER_ROWS = (((0,), (0,)), ((), ()))
MESH = pl.DeviceIdType.MESH
F32, BF16 = jnp.float32, jnp.bfloat16

SIDE = 4
FS = SIDE * SIDE
CHUNK = 256
SLOTS = 3
STEPS = (0, -1, 1, 2)


def kernel(
    tp,
    normed,
    query_cotangent,
    attended,
    output_cotangent,
    query_basis,
    output_basis,
    query_master,
    output_master,
    query_first,
    query_second,
    output_first,
    output_second,
    query_first_new,
    query_second_new,
    query_step,
    query_new,
    query_copy,
    output_first_new,
    output_second_new,
    output_step,
    output_new,
    output_copy,
    gathered,
    tokens,
    basis,
    cotangents,
    master,
    moment,
    lowered,
    partial,
    partial_out,
    partial_in,
    ratio_all,
    square_out,
    square_in,
    block_send,
    block_recv,
    part_send,
    part_recv,
    ratio_send,
    ratio_recv,
    square_send,
    square_recv,
    local_sem,
    token_sem,
    round_sem,
):
    fs_me = lax.axis_index("fs")
    tp_me = lax.axis_index("tp")
    y, x = fs_me // SIDE, fs_me % SIDE
    z, core = tp_me // 2, tp_me % 2
    heights = tp // 2

    def at(dy, dx):
        return ((y + dy + SIDE) % SIDE) * SIDE + (x + dx + SIDE) % SIDE

    def up(dz):
        return ((z + dz + heights) % heights) * 2 + core

    near = [{"fs": at(0, 1)}, {"fs": at(0, -1)}, {"fs": at(1, 0)}, {"fs": at(-1, 0)}]
    near += [{"tp": up(1)}, {"tp": up(-1)}, {"tp": z * 2 + (1 - core)}]

    def greet(sem):
        for device in near:
            pl.semaphore_signal(sem, inc=1, device_id=device, device_id_type=MESH)

    barrier = pltpu.get_barrier_semaphore()
    greet(barrier)

    loads = []
    for k, (src, dst) in enumerate(
        (
            (query_master, master.at[0]),
            (output_master, master.at[1]),
            (query_basis, basis.at[0]),
            (output_basis, basis.at[1]),
            (query_cotangent, cotangents.at[0]),
            (attended, cotangents.at[1]),
            (query_first, moment.at[0]),
            (query_second, moment.at[1]),
            (output_first, moment.at[2]),
            (output_second, moment.at[3]),
        )
    ):
        loads.append(pltpu.make_async_copy(src, dst, local_sem.at[k]))
    for load in loads[:3]:
        load.start()

    chunks = normed.shape[0] // CHUNK
    sources = (normed, output_cotangent)

    def token_load(which, chunk, slot):
        rows = sources[which].at[pl.ds(pl.multiple_of(chunk * CHUNK, CHUNK), CHUNK)]
        return pltpu.make_async_copy(rows, tokens.at[slot], token_sem.at[slot])

    for k in range(SLOTS):
        token_load(0, k, k).start()
    for load in loads[3:]:
        load.start()

    for w in range(2):
        loads[w].wait()
        gathered[w, fs_me] = master[w].astype(BF16)

    half = gathered.shape[2] // 2
    upper, lower, full = pl.ds(0, half), pl.ds(half, half), pl.ds(0, 2 * half)

    def place(w, da, db):
        return at(db, da) if w == 0 else at(da, db)

    def send(w, number, along_a, sign, block, rows):
        device = place(w, sign, 0) if along_a else place(w, 0, sign)
        piece = gathered.at[w, place(w, *block), rows]
        op = pltpu.make_async_remote_copy(
            src_ref=piece,
            dst_ref=piece,
            send_sem=block_send.at[w, number],
            recv_sem=block_recv.at[w, number],
            device_id={"fs": device},
            device_id_type=MESH,
        )
        op.start()
        return op

    sent = []

    def arrived(w, number, block, rows):
        piece = gathered.at[w, place(w, *block), rows]
        pltpu.make_async_remote_copy(
            src_ref=piece,
            dst_ref=piece,
            send_sem=block_send.at[w, number],
            recv_sem=block_recv.at[w, number],
            device_id={"fs": at(0, 1)},
            device_id_type=MESH,
        ).wait_recv()

    def first_own(w):
        sent.append(send(w, 0, True, 1, (0, 0), full))
        sent.append(send(w, 1, True, -1, (0, 0), full))

    def first_relay(w):
        arrived(w, 0, (-1, 0), full)
        sent.append(send(w, 2, True, 1, (-1, 0), upper))
        arrived(w, 1, (1, 0), full)
        sent.append(send(w, 3, True, -1, (1, 0), lower))

    def second_own(w, k):
        if k == 3:
            arrived(w, 2, (2, 0), upper)
            arrived(w, 3, (2, 0), lower)
        sent.append(send(w, 4 + 2 * k, False, 1, (STEPS[k], 0), full))
        sent.append(send(w, 5 + 2 * k, False, -1, (STEPS[k], 0), full))

    def second_relay(w, k):
        arrived(w, 4 + 2 * k, (STEPS[k], -1), full)
        sent.append(send(w, 12 + 2 * k, False, 1, (STEPS[k], -1), upper))
        arrived(w, 5 + 2 * k, (STEPS[k], 1), full)
        sent.append(send(w, 13 + 2 * k, False, -1, (STEPS[k], 1), lower))

    def second_last(w, k):
        arrived(w, 12 + 2 * k, (STEPS[k], 2), upper)
        arrived(w, 13 + 2 * k, (STEPS[k], 2), lower)

    pl.semaphore_wait(barrier, len(near))
    for w in range(2):
        first_own(w)
    for w in range(2):
        second_own(w, 0)

    def project(which, chunk, position):
        slot = lax.rem(position, SLOTS)
        token_load(which, chunk, slot).wait()
        low = jnp.dot(tokens[slot], basis[which], preferred_element_type=F32)
        high = low.astype(BF16)
        rest = (low - high.astype(F32)).astype(BF16)
        rows = pl.ds(pl.multiple_of(chunk * CHUNK, CHUNK), CHUNK)
        rank = low.shape[1]
        lowered[which, rows, pl.ds(0, rank)] = high
        lowered[which, rows, pl.ds(rank, rank)] = rest
        later = position + SLOTS

        @pl.when(later < chunks)
        def _():
            token_load(0, later, slot).start()

        @pl.when(jnp.logical_and(later >= chunks, later < 2 * chunks))
        def _():
            token_load(1, later - chunks, slot).start()

    def pair(which, number):
        greet(round_sem.at[2 * which + number])
        for k in range(2):
            chunk = 2 * number + k
            project(which, chunk, which * chunks + chunk)
        pl.semaphore_wait(round_sem.at[2 * which + number], len(near))

    def finish(which):
        both = lax.dot_general(
            lowered[which], cotangents[which], OVER_ROWS, preferred_element_type=F32
        )
        rank = both.shape[0] // 2
        total = both[:rank] + both[rank:]
        partial[which] = total.reshape(FS, rank // FS, total.shape[1])

    loads[2].wait()

    @pl.loop(0, 2)
    def _(number):
        pair(0, number)

    for load in loads[3:]:
        load.wait()
    finish(0)

    @pl.loop(0, 1)
    def _(number):
        pair(1, number)

    for w in range(2):
        first_relay(w)

    @pl.loop(1, 2)
    def _(number):
        pair(1, number)

    finish(1)
    partial_out[...] = jnp.concatenate([partial[0], partial[1]], axis=1).astype(BF16)

    part_ops = []
    for j in range(1, FS):
        target = lax.rem(fs_me + j, FS)
        op = pltpu.make_async_remote_copy(
            src_ref=partial_out.at[target],
            dst_ref=partial_in.at[j],
            send_sem=part_send.at[j],
            recv_sem=part_recv.at[j],
            device_id={"fs": target},
            device_id_type=MESH,
        )
        op.start()
        part_ops.append(op)

    for w in range(2):
        second_own(w, 1)

    grams = []
    for w in range(2):
        gram = lax.dot_general(basis[w], basis[w], OVER_ROWS, preferred_element_type=F32)
        grams.append(gram)

    for op in part_ops:
        op.wait_recv()
    incoming = jnp.sum(partial_in[pl.ds(1, FS - 1)].astype(F32), axis=0)
    outputs = (
        (query_first_new, query_second_new, query_step, query_new, query_copy),
        (output_first_new, output_second_new, output_step, output_new, output_copy),
    )
    ratios = []
    for w in range(2):
        own = partial[w, fs_me]
        rank_rows = own.shape[0]
        low = own + incoming[w * rank_rows : (w + 1) * rank_rows]
        first_new = FIRST_DECAY * moment[2 * w] + (1.0 - FIRST_DECAY) * low
        second_new = SECOND_DECAY * moment[2 * w + 1] + (1.0 - SECOND_DECAY) * low * low
        outputs[w][0][...] = first_new
        outputs[w][1][...] = second_new
        ratios.append(first_new / jnp.sqrt(second_new + SECOND_FLOOR))
    ratio_all[fs_me] = jnp.concatenate(ratios, axis=0).astype(BF16)

    ratio_ops = []
    for j in range(1, FS):
        op = pltpu.make_async_remote_copy(
            src_ref=ratio_all.at[fs_me],
            dst_ref=ratio_all.at[fs_me],
            send_sem=ratio_send.at[j],
            recv_sem=ratio_recv.at[j],
            device_id={"fs": lax.rem(fs_me + j, FS)},
            device_id_type=MESH,
        )
        op.start()
        ratio_ops.append(op)

    for k in (2, 3):
        for w in range(2):
            second_own(w, k)
    for w in range(2):
        second_relay(w, 0)

    for j in range(1, FS):
        source = lax.rem(fs_me + FS - j, FS)
        pltpu.make_async_remote_copy(
            src_ref=ratio_all.at[source],
            dst_ref=ratio_all.at[source],
            send_sem=ratio_send.at[j],
            recv_sem=ratio_recv.at[j],
            device_id={"fs": lax.rem(fs_me + j, FS)},
            device_id_type=MESH,
        ).wait_recv()
    every = ratio_all[...].astype(F32)
    rank_rows = every.shape[1] // 2
    full_ratio = []
    squares = []
    for w in range(2):
        ratio = every[:, w * rank_rows : (w + 1) * rank_rows, :].reshape(-1, every.shape[2])
        ratio_low = ratio.astype(BF16)
        full_ratio.append(ratio_low)
        high = grams[w].astype(BF16)
        rest = (grams[w] - high.astype(F32)).astype(BF16)
        spread = jnp.dot(high, ratio_low, preferred_element_type=F32)
        spread += jnp.dot(rest, ratio_low, preferred_element_type=F32)
        squares.append(jnp.sum(ratio * spread))
    row = lax.broadcasted_iota(jnp.int32, square_out.shape, 0)
    shares = jnp.where(row < 4, squares[0], squares[1])
    square_out[...] = shares
    square_in[0] = shares

    square_ops = []
    for j in range(1, tp):
        op = pltpu.make_async_remote_copy(
            src_ref=square_out,
            dst_ref=square_in.at[j],
            send_sem=square_send.at[j],
            recv_sem=square_recv.at[j],
            device_id={"tp": lax.rem(tp_me + j, tp)},
            device_id_type=MESH,
        )
        op.start()
        square_ops.append(op)

    for k in (1, 2):
        for w in range(2):
            second_relay(w, k)

    for op in square_ops:
        op.wait_recv()
    entries = basis.shape[1] * full_ratio[0].shape[1] * tp
    factors = lax.rsqrt(jnp.sum(square_in[...], axis=0) / entries + SCALE_FLOOR)
    scale = [factors[0:1, 0:1], factors[4:5, 0:1]]

    block_rows = gathered.shape[2]

    def updated(w, owner):
        rows = pl.ds(pl.multiple_of(owner * block_rows, block_rows), block_rows)
        update = jnp.dot(basis[w, rows], full_ratio[w], preferred_element_type=F32)
        return update * scale[w]

    def settle(w, block):
        owner = place(w, *block)
        step = updated(w, owner)
        new = gathered[w, owner].astype(F32) - LEARN_RATE * step
        outputs[w][4][owner] = new.astype(BF16)

    for w in range(2):
        step = updated(w, fs_me)
        new = master[w] - LEARN_RATE * step
        outputs[w][2][...] = step
        outputs[w][3][...] = new
        outputs[w][4][fs_me] = new.astype(BF16)
        for da in (-1, 1, 2):
            settle(w, (da, 0))
        for k in range(3):
            for db in (-1, 1):
                settle(w, (STEPS[k], db))

    for w in range(2):
        second_relay(w, 3)
    for w in range(2):
        for db in (-1, 1):
            settle(w, (STEPS[3], db))
    for k in range(4):
        for w in range(2):
            second_last(w, k)
            settle(w, (STEPS[k], 2))

    for op in sent + part_ops + ratio_ops + square_ops:
        op.wait_send()


def spread_kernel(count, *refs):
    sources, targets, sem = refs[:count], refs[count : 2 * count], refs[2 * count]
    copies = []
    for k in range(count):
        copies.append(pltpu.make_async_copy(sources[k], targets[k], sem.at[k]))
    for copy in copies:
        copy.start()
    for copy in copies:
        copy.wait()


def body(
    normed,
    query_cotangent,
    attended,
    output_cotangent,
    query_basis,
    output_basis,
    query_master,
    output_master,
    query_first,
    query_second,
    output_first,
    output_second,
):
    operands = (
        normed,
        query_cotangent,
        attended,
        output_cotangent,
        query_basis,
        output_basis,
        query_master,
        output_master,
        query_first,
        query_second,
        output_first,
        output_second,
    )
    tp = lax.axis_size("tp")
    token_rows, width = normed.shape
    rank = query_basis.shape[1]
    rows, columns = query_master.shape
    rank_rows = query_first.shape[0]
    per_weight = (
        ((rank_rows, columns), F32),
        ((rank_rows, columns), F32),
        ((rows, columns), F32),
        ((rows, columns), F32),
        ((FS, rows, columns), BF16),
    )
    results = pl.pallas_call(
        lambda *refs: kernel(tp, *refs),
        out_shape=[pltpu.VMEM(s, d) for s, d in per_weight * 2],
        in_specs=[pl.BlockSpec(memory_space=pltpu.HBM)] * 12,
        out_specs=[pl.BlockSpec(memory_space=pltpu.VMEM)] * 10,
        scratch_shapes=[
            pltpu.VMEM((2, FS, rows, columns), BF16),
            pltpu.VMEM((SLOTS, CHUNK, width), BF16),
            pltpu.VMEM((2, width, rank), BF16),
            pltpu.VMEM((2, token_rows, columns), BF16),
            pltpu.VMEM((2, rows, columns), F32),
            pltpu.VMEM((4, rank_rows, columns), F32),
            pltpu.VMEM((2, token_rows, 2 * rank), BF16),
            pltpu.VMEM((2, FS, rank_rows, columns), F32),
            pltpu.VMEM((FS, 2 * rank_rows, columns), BF16),
            pltpu.VMEM((FS, 2 * rank_rows, columns), BF16),
            pltpu.VMEM((FS, 2 * rank_rows, columns), BF16),
            pltpu.VMEM((8, 128), F32),
            pltpu.VMEM((tp, 8, 128), F32),
            pltpu.SemaphoreType.DMA((2, 20)),
            pltpu.SemaphoreType.DMA((2, 20)),
            pltpu.SemaphoreType.DMA((FS,)),
            pltpu.SemaphoreType.DMA((FS,)),
            pltpu.SemaphoreType.DMA((FS,)),
            pltpu.SemaphoreType.DMA((FS,)),
            pltpu.SemaphoreType.DMA((tp,)),
            pltpu.SemaphoreType.DMA((tp,)),
            pltpu.SemaphoreType.DMA((10,)),
            pltpu.SemaphoreType.DMA((SLOTS,)),
            pltpu.SemaphoreType.REGULAR((4,)),
        ],
        compiler_params=pltpu.CompilerParams(
            collective_id=0, has_side_effects=True, vmem_limit_bytes=40 * 1024 * 1024
        ),
        name="exchange",
    )(*(pltpu.with_memory_space_constraint(operand, pltpu.HBM) for operand in operands))
    count = len(results)
    results = pl.pallas_call(
        lambda *refs: spread_kernel(count, *refs),
        out_shape=[jax.ShapeDtypeStruct(r.shape, r.dtype) for r in results],
        in_specs=[pl.BlockSpec(memory_space=pltpu.VMEM)] * count,
        out_specs=[pl.BlockSpec(memory_space=pl.ANY)] * count,
        scratch_shapes=[pltpu.SemaphoreType.DMA((count,))],
        compiler_params=pltpu.CompilerParams(vmem_limit_bytes=8 * 1024 * 1024),
        name="store",
    )(*results)
    return tuple(r.reshape(-1, columns) for r in results)


def solution(mesh):
    in_specs = (
        P("fs", None),
        P("fs", "tp"),
        P("fs", "tp"),
        P("fs", None),
        P(),
        P(),
        P("fs", "tp"),
        P("fs", "tp"),
        P("fs", "tp"),
        P("fs", "tp"),
        P("fs", "tp"),
        P("fs", "tp"),
    )
    out_specs = (
        P("fs", "tp"),
        P("fs", "tp"),
        P("fs", "tp"),
        P("fs", "tp"),
        P(None, "tp"),
        P("fs", "tp"),
        P("fs", "tp"),
        P("fs", "tp"),
        P("fs", "tp"),
        P(None, "tp"),
    )
    return jax.shard_map(body, mesh=mesh, in_specs=in_specs, out_specs=out_specs, check_vma=False)
```

```python
import jax
import jax.numpy as jnp
from jax import lax
from jax.experimental import pallas as pl
from jax.experimental.pallas import tpu as pltpu
from jax.sharding import PartitionSpec as P

FIRST_DECAY = 0.7
SECOND_DECAY = 0.8
SECOND_FLOOR = 0.05
SCALE_FLOOR = 0.01
LEARN_RATE = 0.05
OVER_ROWS = (((0,), (0,)), ((), ()))
MESH = pl.DeviceIdType.MESH
F32, BF16 = jnp.float32, jnp.bfloat16

SIDE = 4
FS = SIDE * SIDE
CHUNK = 256
UPPER = 128
STEPS = (0, -1, 1, 2)


def kernel(
    tp,
    normed,
    query_cotangent,
    attended,
    output_cotangent,
    query_basis,
    output_basis,
    query_master,
    output_master,
    query_first,
    query_second,
    output_first,
    output_second,
    query_first_new,
    query_second_new,
    query_step,
    query_new,
    query_copy,
    output_first_new,
    output_second_new,
    output_step,
    output_new,
    output_copy,
    gathered,
    tokens,
    basis,
    cotangents,
    master,
    moment,
    lowered,
    partial,
    partial_out,
    partial_in,
    ratio_all,
    update,
    square_out,
    square_in,
    block_send,
    block_recv,
    part_send,
    part_recv,
    ratio_send,
    ratio_recv,
    square_send,
    square_recv,
    half_send,
    half_recv,
    local_sem,
    round_sem,
    entered,
):
    fs_me = lax.axis_index("fs")
    tp_me = lax.axis_index("tp")
    y, x = fs_me // SIDE, fs_me % SIDE
    z, core = tp_me // 2, tp_me % 2
    heights = tp // 2

    def at(dy, dx):
        return ((y + dy + SIDE) % SIDE) * SIDE + (x + dx + SIDE) % SIDE

    def up(dz):
        return ((z + dz + heights) % heights) * 2 + core

    near = [{"fs": at(0, 1)}, {"fs": at(0, -1)}, {"fs": at(1, 0)}, {"fs": at(-1, 0)}]
    partner = {"tp": z * 2 + (1 - core)}

    def tell(sem, device):
        pl.semaphore_signal(sem, inc=1, device_id=device, device_id_type=MESH)

    def greet(sem):
        for device in near:
            tell(sem, device)

    barrier = pltpu.get_barrier_semaphore()
    greet(barrier)
    tell(barrier, partner)
    for dz in range(1, heights):

        @pl.when(z + dz < heights)
        def _():
            for c in range(2):
                tell(barrier, {"tp": (z + dz) * 2 + c})

    sources = (normed, output_cotangent)
    share = normed.shape[0] // 2
    chunks = share // CHUNK

    def token_rows(chunk, of=core):
        return pl.ds(pl.multiple_of(of * share + chunk * CHUNK, CHUNK), CHUNK)

    pieces = [
        (query_master, master.at[0]),
        (output_master, master.at[1]),
        (query_basis, basis.at[0]),
    ]
    for w in range(2):
        for k in range(chunks):
            pieces.append((sources[w].at[token_rows(k)], tokens.at[w, k]))
        if w == 0:
            pieces.append((query_cotangent, cotangents.at[0]))
            pieces.append((output_basis, basis.at[1]))
        else:
            pieces.append((attended, cotangents.at[1]))
    pieces += [
        (query_first, moment.at[0]),
        (query_second, moment.at[1]),
        (output_first, moment.at[2]),
        (output_second, moment.at[3]),
    ]
    loads = []
    for k, (src, dst) in enumerate(pieces):
        loads.append(pltpu.make_async_copy(src, dst, local_sem.at[k]))
        loads[-1].start()

    for w in range(2):
        loads[w].wait()
        gathered[w, fs_me] = master[w].astype(BF16)

    rows = gathered.shape[2]
    upper, lower, full = pl.ds(0, UPPER), pl.ds(UPPER, rows - UPPER), pl.ds(0, rows)

    def place(w, da, db):
        return at(db, da) if w == 0 else at(da, db)

    def send(w, number, along_a, sign, block, rows):
        device = place(w, sign, 0) if along_a else place(w, 0, sign)
        piece = gathered.at[w, place(w, *block), rows]
        op = pltpu.make_async_remote_copy(
            src_ref=piece,
            dst_ref=piece,
            send_sem=block_send.at[w, number],
            recv_sem=block_recv.at[w, number],
            device_id={"fs": device},
            device_id_type=MESH,
        )
        op.start()
        return op

    sent = []

    def arrived(w, number, block, rows):
        piece = gathered.at[w, place(w, *block), rows]
        pltpu.make_async_remote_copy(
            src_ref=piece,
            dst_ref=piece,
            send_sem=block_send.at[w, number],
            recv_sem=block_recv.at[w, number],
            device_id={"fs": at(0, 1)},
            device_id_type=MESH,
        ).wait_recv()

    def first_own(w):
        sent.append(send(w, 0, True, 1, (0, 0), full))
        sent.append(send(w, 1, True, -1, (0, 0), full))

    def first_relay(w):
        arrived(w, 0, (-1, 0), full)
        sent.append(send(w, 2, True, 1, (-1, 0), upper))
        arrived(w, 1, (1, 0), full)
        sent.append(send(w, 3, True, -1, (1, 0), lower))

    def second_own(w, k):
        if k == 3:
            arrived(w, 2, (2, 0), upper)
            arrived(w, 3, (2, 0), lower)
        sent.append(send(w, 4 + 2 * k, False, 1, (STEPS[k], 0), full))
        sent.append(send(w, 5 + 2 * k, False, -1, (STEPS[k], 0), full))

    def second_relay(w, k):
        arrived(w, 4 + 2 * k, (STEPS[k], -1), full)
        sent.append(send(w, 12 + 2 * k, False, 1, (STEPS[k], -1), upper))
        arrived(w, 5 + 2 * k, (STEPS[k], 1), full)
        sent.append(send(w, 13 + 2 * k, False, -1, (STEPS[k], 1), lower))

    def second_last(w, k):
        arrived(w, 12 + 2 * k, (STEPS[k], 2), upper)
        arrived(w, 13 + 2 * k, (STEPS[k], 2), lower)

    pl.semaphore_wait(barrier, len(near) + 1 + 2 * z)
    for w in range(2):
        first_own(w)
    for w in range(2):
        second_own(w, 0)
    greet(round_sem.at[0])
    for dz in range(1, heights):

        @pl.when(z - dz >= 0)
        def _():
            for c in range(2):
                tell(entered, {"tp": (z - dz) * 2 + c})

    halves = []

    def hand_over(w, k, of):
        return pltpu.make_async_remote_copy(
            src_ref=lowered.at[w, token_rows(k, of)],
            dst_ref=lowered.at[w, token_rows(k, of)],
            send_sem=half_send.at[w, k],
            recv_sem=half_recv.at[w, k],
            device_id=partner,
            device_id_type=MESH,
        )

    def project(w, k):
        low = jnp.dot(tokens[w, k], basis[w], preferred_element_type=F32)
        high = low.astype(BF16)
        rest = (low - high.astype(F32)).astype(BF16)
        rank = low.shape[1]
        lowered[w, token_rows(k), pl.ds(0, rank)] = high
        lowered[w, token_rows(k), pl.ds(rank, rank)] = rest
        op = hand_over(w, k, core)
        op.start()
        halves.append(op)

    def finish(w):
        for k in range(chunks):
            hand_over(w, k, 1 - core).wait_recv()
        both = lax.dot_general(
            lowered[w], cotangents[w], OVER_ROWS, preferred_element_type=F32
        )
        rank = both.shape[0] // 2
        total = both[:rank] + both[rank:]
        partial[w] = total.reshape(FS, rank // FS, total.shape[1])

    def next_round(k):
        pl.semaphore_wait(round_sem.at[k], len(near))
        if k < 2:
            greet(round_sem.at[k + 1])

    loads[2].wait()
    loads[3].wait()
    project(0, 0)
    loads[4].wait()
    project(0, 1)
    next_round(0)
    loads[5].wait()
    loads[6].wait()
    loads[7].wait()
    project(1, 0)
    finish(0)
    next_round(1)
    loads[8].wait()
    project(1, 1)
    loads[9].wait()
    finish(1)
    partial_out[...] = jnp.concatenate([partial[0], partial[1]], axis=1).astype(BF16)
    next_round(2)

    part_ops = []
    for j in range(1, FS):
        target = lax.rem(fs_me + j, FS)
        op = pltpu.make_async_remote_copy(
            src_ref=partial_out.at[target],
            dst_ref=partial_in.at[j],
            send_sem=part_send.at[j],
            recv_sem=part_recv.at[j],
            device_id={"fs": target},
            device_id_type=MESH,
        )
        op.start()
        part_ops.append(op)

    for w in range(2):
        first_relay(w)
    for w in range(2):
        second_own(w, 1)

    grams = []
    for w in range(2):
        gram = lax.dot_general(basis[w], basis[w], OVER_ROWS, preferred_element_type=F32)
        grams.append(gram)

    for load in loads[10:]:
        load.wait()
    for op in part_ops:
        op.wait_recv()
    incoming = jnp.sum(partial_in[pl.ds(1, FS - 1)].astype(F32), axis=0)
    outputs = (
        (query_first_new, query_second_new, query_step, query_new, query_copy),
        (output_first_new, output_second_new, output_step, output_new, output_copy),
    )
    ratios = []
    for w in range(2):
        own = partial[w, fs_me]
        rank_rows = own.shape[0]
        low = own + incoming[w * rank_rows : (w + 1) * rank_rows]
        first_new = FIRST_DECAY * moment[2 * w] + (1.0 - FIRST_DECAY) * low
        second_new = SECOND_DECAY * moment[2 * w + 1] + (1.0 - SECOND_DECAY) * low * low
        outputs[w][0][...] = first_new
        outputs[w][1][...] = second_new
        ratios.append(first_new / jnp.sqrt(second_new + SECOND_FLOOR))
    ratio_all[fs_me] = jnp.concatenate(ratios, axis=0).astype(BF16)

    ratio_ops = []
    for j in range(1, FS):
        op = pltpu.make_async_remote_copy(
            src_ref=ratio_all.at[fs_me],
            dst_ref=ratio_all.at[fs_me],
            send_sem=ratio_send.at[j],
            recv_sem=ratio_recv.at[j],
            device_id={"fs": lax.rem(fs_me + j, FS)},
            device_id_type=MESH,
        )
        op.start()
        ratio_ops.append(op)

    for k in (2, 3):
        for w in range(2):
            second_own(w, k)
    for w in range(2):
        second_relay(w, 0)

    for j in range(1, FS):
        source = lax.rem(fs_me + FS - j, FS)
        pltpu.make_async_remote_copy(
            src_ref=ratio_all.at[source],
            dst_ref=ratio_all.at[source],
            send_sem=ratio_send.at[j],
            recv_sem=ratio_recv.at[j],
            device_id={"fs": lax.rem(fs_me + j, FS)},
            device_id_type=MESH,
        ).wait_recv()
    every = ratio_all[...].astype(F32)
    rank_rows = every.shape[1] // 2
    full_ratio = []
    squares = []
    for w in range(2):
        ratio = every[:, w * rank_rows : (w + 1) * rank_rows, :].reshape(-1, every.shape[2])
        ratio_low = ratio.astype(BF16)
        full_ratio.append(ratio_low)
        high = grams[w].astype(BF16)
        rest = (grams[w] - high.astype(F32)).astype(BF16)
        spread = jnp.dot(high, ratio_low, preferred_element_type=F32)
        spread += jnp.dot(rest, ratio_low, preferred_element_type=F32)
        squares.append(jnp.sum(ratio * spread))
    row = lax.broadcasted_iota(jnp.int32, square_out.shape, 0)
    shares = jnp.where(row < 4, squares[0], squares[1])
    square_out[...] = shares
    square_in[0] = shares

    @pl.when(z < heights - 1)
    def _():
        pl.semaphore_wait(entered, 2 * (heights - 1 - z))

    square_ops = []
    for j in range(1, tp):
        op = pltpu.make_async_remote_copy(
            src_ref=square_out,
            dst_ref=square_in.at[j],
            send_sem=square_send.at[j],
            recv_sem=square_recv.at[j],
            device_id={"tp": lax.rem(tp_me + j, tp)},
            device_id_type=MESH,
        )
        op.start()
        square_ops.append(op)

    @pl.loop(0, FS // 2)
    def _(k):
        for w in range(2):
            pair = pl.ds(pl.multiple_of(2 * rows * k, 2 * rows), 2 * rows)
            product = jnp.dot(basis[w, pair], full_ratio[w], preferred_element_type=F32)
            update[w, pl.ds(2 * k, 2)] = product.reshape(2, rows, product.shape[1])

    for k in (1, 2, 3):
        for w in range(2):
            second_relay(w, k)

    for op in square_ops:
        op.wait_recv()
    entries = basis.shape[1] * full_ratio[0].shape[1] * tp
    factors = lax.rsqrt(jnp.sum(square_in[...], axis=0) / entries + SCALE_FLOOR)
    scale = [factors[0:1, 0:1], factors[4:5, 0:1]]

    def settle(w, da, db):
        owner = place(w, da, db)
        new = gathered[w, owner].astype(F32) - (LEARN_RATE * scale[w]) * update[w, owner]
        outputs[w][4][owner] = new.astype(BF16)

    @pl.loop(1, 3 * SIDE)
    def _(k):
        db = lax.rem(k // SIDE + 1, 3) - 1
        for w in range(2):
            settle(w, lax.rem(k, SIDE), db)

    for w in range(2):
        step = update[w, fs_me] * scale[w]
        new = master[w] - LEARN_RATE * step
        outputs[w][2][...] = step
        outputs[w][3][...] = new
        outputs[w][4][fs_me] = new.astype(BF16)

    for k in range(4):
        for w in range(2):
            second_last(w, k)
            settle(w, STEPS[k], 2)

    for op in sent + halves + part_ops + ratio_ops + square_ops:
        op.wait_send()


def store_kernel(count, *refs):
    sources, targets, sem = refs[:count], refs[count : 2 * count], refs[2 * count]
    copies = []
    for k in range(count):
        pieces = 4 if len(sources[k].shape) == 3 else 1
        size = sources[k].shape[0] // pieces
        for p in range(pieces):
            part = pl.ds(p * size, size)
            copies.append(
                pltpu.make_async_copy(sources[k].at[part], targets[k].at[part], sem.at[len(copies)])
            )
            copies[-1].start()
    for copy in copies:
        copy.wait()


def body(
    normed,
    query_cotangent,
    attended,
    output_cotangent,
    query_basis,
    output_basis,
    query_master,
    output_master,
    query_first,
    query_second,
    output_first,
    output_second,
):
    operands = (
        normed,
        query_cotangent,
        attended,
        output_cotangent,
        query_basis,
        output_basis,
        query_master,
        output_master,
        query_first,
        query_second,
        output_first,
        output_second,
    )
    tp = lax.axis_size("tp")
    token_rows, width = normed.shape
    rank = query_basis.shape[1]
    rows, columns = query_master.shape
    rank_rows = query_first.shape[0]
    per_weight = (
        ((rank_rows, columns), F32),
        ((rank_rows, columns), F32),
        ((rows, columns), F32),
        ((rows, columns), F32),
        ((FS, rows, columns), BF16),
    )
    results = pl.pallas_call(
        lambda *refs: kernel(tp, *refs),
        out_shape=[pltpu.VMEM(s, d) for s, d in per_weight * 2],
        in_specs=[pl.BlockSpec(memory_space=pltpu.HBM)] * 12,
        out_specs=[pl.BlockSpec(memory_space=pltpu.VMEM)] * 10,
        scratch_shapes=[
            pltpu.VMEM((2, FS, rows, columns), BF16),
            pltpu.VMEM((2, token_rows // 2 // CHUNK, CHUNK, width), BF16),
            pltpu.VMEM((2, width, rank), BF16),
            pltpu.VMEM((2, token_rows, columns), BF16),
            pltpu.VMEM((2, rows, columns), F32),
            pltpu.VMEM((4, rank_rows, columns), F32),
            pltpu.VMEM((2, token_rows, 2 * rank), BF16),
            pltpu.VMEM((2, FS, rank_rows, columns), F32),
            pltpu.VMEM((FS, 2 * rank_rows, columns), BF16),
            pltpu.VMEM((FS, 2 * rank_rows, columns), BF16),
            pltpu.VMEM((FS, 2 * rank_rows, columns), BF16),
            pltpu.VMEM((2, FS, rows, columns), F32),
            pltpu.VMEM((8, 128), F32),
            pltpu.VMEM((tp, 8, 128), F32),
            pltpu.SemaphoreType.DMA((2, 20)),
            pltpu.SemaphoreType.DMA((2, 20)),
            pltpu.SemaphoreType.DMA((FS,)),
            pltpu.SemaphoreType.DMA((FS,)),
            pltpu.SemaphoreType.DMA((FS,)),
            pltpu.SemaphoreType.DMA((FS,)),
            pltpu.SemaphoreType.DMA((tp,)),
            pltpu.SemaphoreType.DMA((tp,)),
            pltpu.SemaphoreType.DMA((2, token_rows // 2 // CHUNK)),
            pltpu.SemaphoreType.DMA((2, token_rows // 2 // CHUNK)),
            pltpu.SemaphoreType.DMA((14,)),
            pltpu.SemaphoreType.REGULAR((3,)),
            pltpu.SemaphoreType.REGULAR,
        ],
        compiler_params=pltpu.CompilerParams(
            collective_id=0, has_side_effects=True, vmem_limit_bytes=40 * 1024 * 1024
        ),
        name="exchange",
    )(*(pltpu.with_memory_space_constraint(operand, pltpu.HBM) for operand in operands))
    count = len(results)
    results = pl.pallas_call(
        lambda *refs: store_kernel(count, *refs),
        out_shape=[jax.ShapeDtypeStruct(r.shape, r.dtype) for r in results],
        in_specs=[pl.BlockSpec(memory_space=pltpu.VMEM)] * count,
        out_specs=[pl.BlockSpec(memory_space=pl.ANY)] * count,
        scratch_shapes=[pltpu.SemaphoreType.DMA((2 * count,))],
        compiler_params=pltpu.CompilerParams(vmem_limit_bytes=8 * 1024 * 1024),
        name="store",
    )(*results)
    return tuple(r.reshape(-1, columns) for r in results)


def solution(mesh):
    in_specs = (
        P("fs", None),
        P("fs", "tp"),
        P("fs", "tp"),
        P("fs", None),
        P(),
        P(),
        P("fs", "tp"),
        P("fs", "tp"),
        P("fs", "tp"),
        P("fs", "tp"),
        P("fs", "tp"),
        P("fs", "tp"),
    )
    out_specs = (
        P("fs", "tp"),
        P("fs", "tp"),
        P("fs", "tp"),
        P("fs", "tp"),
        P(None, "tp"),
        P("fs", "tp"),
        P("fs", "tp"),
        P("fs", "tp"),
        P("fs", "tp"),
        P(None, "tp"),
    )
    return jax.shard_map(body, mesh=mesh, in_specs=in_specs, out_specs=out_specs, check_vma=False)
```

```python
import jax
import jax.numpy as jnp
from jax import lax
from jax.experimental import pallas as pl
from jax.experimental.pallas import tpu as pltpu
from jax.sharding import PartitionSpec as P

FIRST_DECAY = 0.7
SECOND_DECAY = 0.8
SECOND_FLOOR = 0.05
SCALE_FLOOR = 0.01
LEARN_RATE = 0.05
OVER_ROWS = (((0,), (0,)), ((), ()))
MESH = pl.DeviceIdType.MESH
F32, BF16 = jnp.float32, jnp.bfloat16

SIDE = 4
FS = SIDE * SIDE
CHUNK = 128
UPPER = 128
STEPS = (0, -1, 1, 2)


def kernel(
    tp,
    normed,
    query_cotangent,
    attended,
    output_cotangent,
    query_basis,
    output_basis,
    query_master,
    output_master,
    query_first,
    query_second,
    output_first,
    output_second,
    gathered,
    update,
    own_update,
    master,
    scales,
    query_first_new,
    query_second_new,
    output_first_new,
    output_second_new,
    tokens,
    basis,
    cotangents,
    moment,
    lowered,
    partial,
    partial_out,
    partial_in,
    ratio_all,
    square_out,
    square_in,
    block_send,
    block_recv,
    part_send,
    part_recv,
    ratio_send,
    ratio_recv,
    square_send,
    square_recv,
    half_send,
    half_recv,
    local_sem,
    round_sem,
    entered,
):
    fs_me = lax.axis_index("fs")
    tp_me = lax.axis_index("tp")
    y, x = fs_me // SIDE, fs_me % SIDE
    z, core = tp_me // 2, tp_me % 2
    heights = tp // 2

    def at(dy, dx):
        return ((y + dy + SIDE) % SIDE) * SIDE + (x + dx + SIDE) % SIDE

    def up(dz):
        return ((z + dz + heights) % heights) * 2 + core

    near = [{"fs": at(0, 1)}, {"fs": at(0, -1)}, {"fs": at(1, 0)}, {"fs": at(-1, 0)}]
    partner = {"tp": z * 2 + (1 - core)}

    def tell(sem, device):
        pl.semaphore_signal(sem, inc=1, device_id=device, device_id_type=MESH)

    def greet(sem):
        for device in near:
            tell(sem, device)

    barrier = pltpu.get_barrier_semaphore()
    greet(barrier)
    tell(barrier, partner)
    for dz in range(1, heights):

        @pl.when(z + dz < heights)
        def _():
            for c in range(2):
                tell(barrier, {"tp": (z + dz) * 2 + c})

    sources = (normed, output_cotangent)
    share = normed.shape[0] // 2
    chunks = share // CHUNK

    def token_rows(chunk, of=core):
        return pl.ds(pl.multiple_of(of * share + chunk * CHUNK, CHUNK), CHUNK)

    pieces = [
        (query_master, master.at[0]),
        (output_master, master.at[1]),
        (query_basis, basis.at[0]),
    ]
    for w in range(2):
        for k in range(chunks):
            pieces.append((sources[w].at[token_rows(k)], tokens.at[w, k]))
        if w == 0:
            pieces.append((query_cotangent, cotangents.at[0]))
            pieces.append((output_basis, basis.at[1]))
        else:
            pieces.append((attended, cotangents.at[1]))
    pieces += [
        (query_first, moment.at[0]),
        (query_second, moment.at[1]),
        (output_first, moment.at[2]),
        (output_second, moment.at[3]),
    ]
    loads = []
    for k, (src, dst) in enumerate(pieces):
        loads.append(pltpu.make_async_copy(src, dst, local_sem.at[k]))
        loads[-1].start()

    for w in range(2):
        loads[w].wait()
        gathered[w, fs_me] = master[w].astype(BF16)

    rows = gathered.shape[2]
    upper, lower, full = pl.ds(0, UPPER), pl.ds(UPPER, rows - UPPER), pl.ds(0, rows)

    def place(w, da, db):
        return at(db, da) if w == 0 else at(da, db)

    def send(w, number, along_a, sign, block, rows):
        device = place(w, sign, 0) if along_a else place(w, 0, sign)
        piece = gathered.at[w, place(w, *block), rows]
        op = pltpu.make_async_remote_copy(
            src_ref=piece,
            dst_ref=piece,
            send_sem=block_send.at[w],
            recv_sem=block_recv.at[w, number],
            device_id={"fs": device},
            device_id_type=MESH,
        )
        op.start()

    def arrived(w, number, block, rows):
        piece = gathered.at[w, place(w, *block), rows]
        pltpu.make_async_remote_copy(
            src_ref=piece,
            dst_ref=piece,
            send_sem=block_send.at[w],
            recv_sem=block_recv.at[w, number],
            device_id={"fs": at(0, 1)},
            device_id_type=MESH,
        ).wait_recv()

    def first_own(w):
        send(w, 0, True, 1, (0, 0), full)
        send(w, 1, True, -1, (0, 0), full)

    def first_relay(w):
        arrived(w, 0, (-1, 0), full)
        send(w, 2, True, 1, (-1, 0), upper)
        arrived(w, 1, (1, 0), full)
        send(w, 3, True, -1, (1, 0), lower)

    def second_own(w, k):
        if k == 3:
            arrived(w, 2, (2, 0), upper)
            arrived(w, 3, (2, 0), lower)
        send(w, 4 + 2 * k, False, 1, (STEPS[k], 0), full)
        send(w, 5 + 2 * k, False, -1, (STEPS[k], 0), full)

    def second_relay(w, k):
        arrived(w, 4 + 2 * k, (STEPS[k], -1), full)
        send(w, 12 + 2 * k, False, 1, (STEPS[k], -1), upper)
        arrived(w, 5 + 2 * k, (STEPS[k], 1), full)
        send(w, 13 + 2 * k, False, -1, (STEPS[k], 1), lower)

    def second_last(w, k):
        arrived(w, 12 + 2 * k, (STEPS[k], 2), upper)
        arrived(w, 13 + 2 * k, (STEPS[k], 2), lower)

    pl.semaphore_wait(barrier, len(near) + 1 + 2 * z)
    for w in range(2):
        first_own(w)
    for w in range(2):
        second_own(w, 0)
    greet(round_sem.at[0])
    for dz in range(1, heights):

        @pl.when(z - dz >= 0)
        def _():
            for c in range(2):
                tell(entered, {"tp": (z - dz) * 2 + c})

    def hand_over(w, k, of):
        return pltpu.make_async_remote_copy(
            src_ref=lowered.at[w, token_rows(k, of)],
            dst_ref=lowered.at[w, token_rows(k, of)],
            send_sem=half_send,
            recv_sem=half_recv.at[w, k],
            device_id=partner,
            device_id_type=MESH,
        )

    def project(w, k):
        low = jnp.dot(tokens[w, k], basis[w], preferred_element_type=F32)
        high = low.astype(BF16)
        rest = (low - high.astype(F32)).astype(BF16)
        rank = low.shape[1]
        lowered[w, token_rows(k), pl.ds(0, rank)] = high
        lowered[w, token_rows(k), pl.ds(rank, rank)] = rest
        op = hand_over(w, k, core)
        op.start()

    def contract(w, of):
        half = pl.ds(pl.multiple_of(of * share, share), share)
        return lax.dot_general(
            lowered[w, half], cotangents[w, half], OVER_ROWS, preferred_element_type=F32
        )

    def finish(w):
        both = contract(w, core)
        for k in range(chunks):
            hand_over(w, k, 1 - core).wait_recv()
        both += contract(w, 1 - core)
        rank = both.shape[0] // 2
        total = both[:rank] + both[rank:]
        partial[w] = total.reshape(FS, rank // FS, total.shape[1])

    def next_round(k):
        pl.semaphore_wait(round_sem.at[k], len(near))
        if k < 2:
            greet(round_sem.at[k + 1])

    loads[2].wait()
    first = 3
    for w in range(2):
        if w == 1:
            loads[first].wait()
            loads[first + 1].wait()
            first += 2
        for k in range(chunks):
            loads[first + k].wait()
            project(w, k)
            if w == 1 and k == 0:
                next_round(0)
                finish(0)
            if w == 1 and k == 2:
                next_round(1)
        first += chunks
    loads[first].wait()
    finish(1)
    first += 1
    partial_out[...] = jnp.concatenate([partial[0], partial[1]], axis=1).astype(BF16)
    next_round(2)

    for j in range(1, FS):
        target = lax.rem(fs_me + j, FS)
        op = pltpu.make_async_remote_copy(
            src_ref=partial_out.at[target],
            dst_ref=partial_in.at[j],
            send_sem=part_send,
            recv_sem=part_recv,
            device_id={"fs": target},
            device_id_type=MESH,
        )
        op.start()

    for w in range(2):
        first_relay(w)
    for w in range(2):
        second_own(w, 1)

    grams = []
    for w in range(2):
        gram = lax.dot_general(basis[w], basis[w], OVER_ROWS, preferred_element_type=F32)
        grams.append(gram)

    for load in loads[first:]:
        load.wait()
    def together(refs, sems):
        return pltpu.make_async_remote_copy(
            src_ref=refs,
            dst_ref=refs,
            send_sem=sems[0],
            recv_sem=sems[1],
            device_id=partner,
            device_id_type=MESH,
        )

    others = pl.ds(1, FS - 1)
    parts = together(partial_in.at[others], (part_send, part_recv))
    parts.wait_recv()
    incoming = jnp.sum(partial_in[pl.ds(1, FS - 1)].astype(F32), axis=0)
    moments = (
        (query_first_new, query_second_new),
        (output_first_new, output_second_new),
    )
    ratios = []
    for w in range(2):
        own = partial[w, fs_me]
        rank_rows = own.shape[0]
        low = own + incoming[w * rank_rows : (w + 1) * rank_rows]
        first_new = FIRST_DECAY * moment[2 * w] + (1.0 - FIRST_DECAY) * low
        second_new = SECOND_DECAY * moment[2 * w + 1] + (1.0 - SECOND_DECAY) * low * low
        moments[w][0][...] = first_new
        moments[w][1][...] = second_new
        ratios.append(first_new / jnp.sqrt(second_new + SECOND_FLOOR))
    ratio_all[fs_me] = jnp.concatenate(ratios, axis=0).astype(BF16)

    for j in range(1, FS):
        op = pltpu.make_async_remote_copy(
            src_ref=ratio_all.at[fs_me],
            dst_ref=ratio_all.at[fs_me],
            send_sem=ratio_send,
            recv_sem=ratio_recv,
            device_id={"fs": lax.rem(fs_me + j, FS)},
            device_id_type=MESH,
        )
        op.start()

    for k in (2, 3):
        for w in range(2):
            second_own(w, k)
    for w in range(2):
        second_relay(w, 0)

    shared = together(ratio_all.at[others], (ratio_send, ratio_recv))
    shared.wait_recv()
    every = ratio_all[...].astype(F32)
    rank_rows = every.shape[1] // 2
    full_ratio = []
    squares = []
    for w in range(2):
        ratio = every[:, w * rank_rows : (w + 1) * rank_rows, :].reshape(-1, every.shape[2])
        ratio_low = ratio.astype(BF16)
        full_ratio.append(ratio_low)
        high = grams[w].astype(BF16)
        rest = (grams[w] - high.astype(F32)).astype(BF16)
        spread = jnp.dot(high, ratio_low, preferred_element_type=F32)
        spread += jnp.dot(rest, ratio_low, preferred_element_type=F32)
        squares.append(jnp.sum(ratio * spread))
    lane = lax.broadcasted_iota(jnp.int32, square_out.shape, 1)
    shares = jnp.where(lane < square_out.shape[1] // 2, squares[0], squares[1])
    square_out[...] = shares
    square_in[0] = shares

    @pl.when(z < heights - 1)
    def _():
        pl.semaphore_wait(entered, 2 * (heights - 1 - z))

    for j in range(1, tp):
        op = pltpu.make_async_remote_copy(
            src_ref=square_out,
            dst_ref=square_in.at[j],
            send_sem=square_send,
            recv_sem=square_recv,
            device_id={"tp": lax.rem(tp_me + j, tp)},
            device_id_type=MESH,
        )
        op.start()

    @pl.loop(0, FS // 2)
    def _(k):
        for w in range(2):
            pair = pl.ds(pl.multiple_of(2 * rows * k, 2 * rows), 2 * rows)
            product = jnp.dot(basis[w, pair], full_ratio[w], preferred_element_type=F32)
            product = product.reshape(2, rows, product.shape[1])
            update[w, pl.ds(2 * k, 2)] = product.astype(BF16)

    for k in (1, 2):
        for w in range(2):
            second_relay(w, k)
    own_rows = pl.ds(pl.multiple_of(fs_me * rows, rows), rows)
    for w in range(2):
        own_update[w] = jnp.dot(
            basis[w, own_rows], full_ratio[w], preferred_element_type=F32
        )
    for w in range(2):
        second_relay(w, 3)

    totals = together(square_in.at[pl.ds(1, tp - 1)], (square_send, square_recv))
    totals.wait_recv()
    entries = basis.shape[1] * full_ratio[0].shape[1] * tp
    factors = lax.rsqrt(jnp.sum(square_in[...], axis=0) / entries + SCALE_FLOOR)
    scales[...] = factors

    own_share = lowered.at[:, pl.ds(0, share)]
    together(own_share, (half_send, half_recv.at[0, 0])).wait_send()
    parts.wait_send()
    shared.wait_send()
    totals.wait_send()
    for k in range(4):
        for w in range(2):
            second_last(w, k)
    for w in range(2):
        together(gathered.at[w, others], (block_send.at[w], block_recv.at[w, 0])).wait_send()


def store_kernel(
    gathered,
    update,
    own_update,
    master,
    scales,
    query_first,
    query_second,
    output_first,
    output_second,
    query_first_new,
    query_second_new,
    query_step,
    query_new,
    query_copy,
    output_first_new,
    output_second_new,
    output_step,
    output_new,
    output_copy,
    copies,
    steps,
    news,
    copy_sem,
    other_sem,
):
    fs_me = lax.axis_index("fs")
    moments = ((query_first, query_second), (output_first, output_second))
    outputs = (
        (query_first_new, query_second_new, query_step, query_new, query_copy),
        (output_first_new, output_second_new, output_step, output_new, output_copy),
    )
    half = scales.shape[1] // 2
    scale = [scales[0:1, 0:1], scales[0:1, half : half + 1]]
    rate = [(LEARN_RATE * scale[w]).astype(BF16) for w in range(2)]

    def copy_out(w, j):
        owner = lax.rem(fs_me + j, FS)
        return pltpu.make_async_copy(
            copies.at[w, owner], outputs[w][4].at[owner], copy_sem.at[w]
        )

    others = []

    def put(w, number, source):
        others.append(pltpu.make_async_copy(source, outputs[w][number], other_sem.at[w, number]))
        others[-1].start()

    @pl.loop(1, FS)
    def _(j):
        owner = lax.rem(fs_me + j, FS)
        for w in range(2):
            copies[w, owner] = gathered[w, owner] - rate[w] * update[w, owner]
            copy_out(w, j).start()

    for w in range(2):
        put(w, 0, moments[w][0])
        put(w, 1, moments[w][1])
        step = own_update[w] * scale[w]
        new = master[w] - LEARN_RATE * step
        steps[w] = step
        put(w, 2, steps.at[w])
        news[w] = new
        put(w, 3, news.at[w])
        copies[w, fs_me] = new.astype(BF16)
        copy_out(w, 0).start()

    for w in range(2):
        pltpu.make_async_copy(copies.at[w], outputs[w][4], copy_sem.at[w]).wait()
    for copy in others:
        copy.wait()


def body(
    normed,
    query_cotangent,
    attended,
    output_cotangent,
    query_basis,
    output_basis,
    query_master,
    output_master,
    query_first,
    query_second,
    output_first,
    output_second,
):
    operands = (
        normed,
        query_cotangent,
        attended,
        output_cotangent,
        query_basis,
        output_basis,
        query_master,
        output_master,
        query_first,
        query_second,
        output_first,
        output_second,
    )
    tp = lax.axis_size("tp")
    token_rows, width = normed.shape
    rank = query_basis.shape[1]
    rows, columns = query_master.shape
    rank_rows = query_first.shape[0]
    blocks, block, small = (2, FS, rows, columns), (2, rows, columns), (rank_rows, columns)
    pieces = token_rows // 2 // CHUNK
    exchanged = pl.pallas_call(
        lambda *refs: kernel(tp, *refs),
        out_shape=[
            pltpu.VMEM(blocks, BF16),
            pltpu.VMEM(blocks, BF16),
            pltpu.VMEM(block, F32),
            pltpu.VMEM(block, F32),
            pltpu.VMEM((1, 128), F32),
            pltpu.VMEM(small, F32),
            pltpu.VMEM(small, F32),
            pltpu.VMEM(small, F32),
            pltpu.VMEM(small, F32),
        ],
        in_specs=[pl.BlockSpec(memory_space=pltpu.HBM)] * 12,
        out_specs=[pl.BlockSpec(memory_space=pltpu.VMEM)] * 9,
        scratch_shapes=[
            pltpu.VMEM((2, pieces, CHUNK, width), BF16),
            pltpu.VMEM((2, width, rank), BF16),
            pltpu.VMEM((2, token_rows, columns), BF16),
            pltpu.VMEM((4, rank_rows, columns), F32),
            pltpu.VMEM((2, token_rows, 2 * rank), BF16),
            pltpu.VMEM((2, FS, rank_rows, columns), F32),
            pltpu.VMEM((FS, 2 * rank_rows, columns), BF16),
            pltpu.VMEM((FS, 2 * rank_rows, columns), BF16),
            pltpu.VMEM((FS, 2 * rank_rows, columns), BF16),
            pltpu.VMEM((1, 128), F32),
            pltpu.VMEM((tp, 1, 128), F32),
            pltpu.SemaphoreType.DMA((2,)),
            pltpu.SemaphoreType.DMA((2, 20)),
            pltpu.SemaphoreType.DMA,
            pltpu.SemaphoreType.DMA,
            pltpu.SemaphoreType.DMA,
            pltpu.SemaphoreType.DMA,
            pltpu.SemaphoreType.DMA,
            pltpu.SemaphoreType.DMA,
            pltpu.SemaphoreType.DMA,
            pltpu.SemaphoreType.DMA((2, pieces)),
            pltpu.SemaphoreType.DMA((10 + 2 * pieces,)),
            pltpu.SemaphoreType.REGULAR((3,)),
            pltpu.SemaphoreType.REGULAR,
        ],
        compiler_params=pltpu.CompilerParams(
            collective_id=0, has_side_effects=True, vmem_limit_bytes=28 * 1024 * 1024
        ),
        name="exchange",
    )(*(pltpu.with_memory_space_constraint(operand, pltpu.HBM) for operand in operands))
    per_weight = (
        jax.ShapeDtypeStruct(small, F32),
        jax.ShapeDtypeStruct(small, F32),
        jax.ShapeDtypeStruct((rows, columns), F32),
        jax.ShapeDtypeStruct((rows, columns), F32),
        jax.ShapeDtypeStruct((FS, rows, columns), BF16),
    )
    results = pl.pallas_call(
        store_kernel,
        out_shape=per_weight * 2,
        in_specs=[pl.BlockSpec(memory_space=pltpu.VMEM)] * 9,
        out_specs=[pl.BlockSpec(memory_space=pl.ANY)] * 10,
        scratch_shapes=[
            pltpu.VMEM(blocks, BF16),
            pltpu.VMEM(block, F32),
            pltpu.VMEM(block, F32),
            pltpu.SemaphoreType.DMA((2,)),
            pltpu.SemaphoreType.DMA((2, 4)),
        ],
        compiler_params=pltpu.CompilerParams(vmem_limit_bytes=16 * 1024 * 1024),
        name="store",
    )(*exchanged)
    return tuple(r.reshape(-1, columns) for r in results)


def solution(mesh):
    in_specs = (
        P("fs", None),
        P("fs", "tp"),
        P("fs", "tp"),
        P("fs", None),
        P(),
        P(),
        P("fs", "tp"),
        P("fs", "tp"),
        P("fs", "tp"),
        P("fs", "tp"),
        P("fs", "tp"),
        P("fs", "tp"),
    )
    out_specs = (
        P("fs", "tp"),
        P("fs", "tp"),
        P("fs", "tp"),
        P("fs", "tp"),
        P(None, "tp"),
        P("fs", "tp"),
        P("fs", "tp"),
        P("fs", "tp"),
        P("fs", "tp"),
        P(None, "tp"),
    )
    return jax.shard_map(body, mesh=mesh, in_specs=in_specs, out_specs=out_specs, check_vma=False)
```

```python
import jax
import jax.numpy as jnp
from jax import lax
from jax.experimental import pallas as pl
from jax.experimental.pallas import tpu as pltpu
from jax.sharding import PartitionSpec as P

FIRST_DECAY = 0.7
SECOND_DECAY = 0.8
SECOND_FLOOR = 0.05
SCALE_FLOOR = 0.01
LEARN_RATE = 0.05
OVER_ROWS = (((0,), (0,)), ((), ()))
MESH = pl.DeviceIdType.MESH
F32, BF16 = jnp.float32, jnp.bfloat16

SIDE = 4
FS = SIDE * SIDE
CHUNK = 128
UPPER = 112
STEPS = (0, -1, 1, 2)


def kernel(
    tp,
    normed,
    query_cotangent,
    attended,
    output_cotangent,
    query_basis,
    output_basis,
    query_master,
    output_master,
    query_first,
    query_second,
    output_first,
    output_second,
    gathered,
    update,
    own_update,
    master,
    scales,
    query_first_new,
    query_second_new,
    output_first_new,
    output_second_new,
    tokens,
    basis,
    cotangents,
    moment,
    lowered,
    partial,
    partial_out,
    partial_in,
    ratio_all,
    square_out,
    square_in,
    block_send,
    block_recv,
    part_send,
    part_recv,
    ratio_send,
    ratio_recv,
    square_send,
    square_recv,
    half_send,
    half_recv,
    local_sem,
    round_sem,
    entered,
):
    fs_me = lax.axis_index("fs")
    tp_me = lax.axis_index("tp")
    y, x = fs_me // SIDE, fs_me % SIDE
    z, core = tp_me // 2, tp_me % 2
    heights = tp // 2

    def at(dy, dx):
        return ((y + dy + SIDE) % SIDE) * SIDE + (x + dx + SIDE) % SIDE

    def up(dz):
        return ((z + dz + heights) % heights) * 2 + core

    near = [{"fs": at(0, 1)}, {"fs": at(0, -1)}, {"fs": at(1, 0)}, {"fs": at(-1, 0)}]
    partner = {"tp": z * 2 + (1 - core)}

    def tell(sem, device):
        pl.semaphore_signal(sem, inc=1, device_id=device, device_id_type=MESH)

    def greet(sem):
        for device in near:
            tell(sem, device)

    sources = (normed, output_cotangent)
    share = normed.shape[0] // 2
    chunks = share // CHUNK

    def token_rows(chunk, of=core):
        return pl.ds(pl.multiple_of(of * share + chunk * CHUNK, CHUNK), CHUNK)

    pieces = [
        (query_master, master.at[0]),
        (output_master, master.at[1]),
        (query_basis, basis.at[0]),
    ]
    for w in range(2):
        for k in range(chunks):
            pieces.append((sources[w].at[token_rows(k)], tokens.at[w, k]))
        if w == 0:
            pieces.append((query_cotangent, cotangents.at[0]))
            pieces.append((output_basis, basis.at[1]))
        else:
            pieces.append((attended, cotangents.at[1]))
    pieces += [
        (query_first, moment.at[0]),
        (query_second, moment.at[1]),
        (output_first, moment.at[2]),
        (output_second, moment.at[3]),
    ]
    loads = []
    for k, (src, dst) in enumerate(pieces):
        loads.append(pltpu.make_async_copy(src, dst, local_sem.at[k]))
    for load in loads[:2]:
        load.start()

    barrier = pltpu.get_barrier_semaphore()
    greet(barrier)
    tell(barrier, partner)
    for dz in range(1, heights):

        @pl.when(z + dz < heights)
        def _():
            for c in range(2):
                tell(barrier, {"tp": (z + dz) * 2 + c})

    for load in loads[2:]:
        load.start()

    for w in range(2):
        loads[w].wait()
        gathered[w, fs_me] = master[w].astype(BF16)

    rows = gathered.shape[2]
    upper, lower, full = pl.ds(0, UPPER), pl.ds(UPPER, rows - UPPER), pl.ds(0, rows)

    def place(w, da, db):
        return at(db, da) if w == 0 else at(da, db)

    def send(w, number, along_a, sign, block, rows):
        device = place(w, sign, 0) if along_a else place(w, 0, sign)
        piece = gathered.at[w, place(w, *block), rows]
        op = pltpu.make_async_remote_copy(
            src_ref=piece,
            dst_ref=piece,
            send_sem=block_send.at[w],
            recv_sem=block_recv.at[w, number],
            device_id={"fs": device},
            device_id_type=MESH,
        )
        op.start()

    def arrived(w, number, block, rows):
        piece = gathered.at[w, place(w, *block), rows]
        pltpu.make_async_remote_copy(
            src_ref=piece,
            dst_ref=piece,
            send_sem=block_send.at[w],
            recv_sem=block_recv.at[w, number],
            device_id={"fs": at(0, 1)},
            device_id_type=MESH,
        ).wait_recv()

    def first_own(w):
        send(w, 0, True, 1, (0, 0), full)
        send(w, 1, True, -1, (0, 0), full)

    def first_relay(w):
        arrived(w, 0, (-1, 0), full)
        send(w, 2, True, 1, (-1, 0), upper)
        arrived(w, 1, (1, 0), full)
        send(w, 3, True, -1, (1, 0), lower)

    def second_own(w, k):
        if k == 3:
            arrived(w, 2, (2, 0), upper)
            arrived(w, 3, (2, 0), lower)
        send(w, 4 + 2 * k, False, 1, (STEPS[k], 0), full)
        send(w, 5 + 2 * k, False, -1, (STEPS[k], 0), full)

    def second_relay(w, k):
        arrived(w, 4 + 2 * k, (STEPS[k], -1), full)
        send(w, 12 + 2 * k, False, 1, (STEPS[k], -1), upper)
        arrived(w, 5 + 2 * k, (STEPS[k], 1), full)
        send(w, 13 + 2 * k, False, -1, (STEPS[k], 1), lower)

    def second_last(w, k):
        arrived(w, 12 + 2 * k, (STEPS[k], 2), upper)
        arrived(w, 13 + 2 * k, (STEPS[k], 2), lower)

    pl.semaphore_wait(barrier, len(near) + 1 + 2 * z)
    for w in range(2):
        first_own(w)
    for w in range(2):
        second_own(w, 0)
    greet(round_sem.at[0])
    for dz in range(1, heights):

        @pl.when(z - dz >= 0)
        def _():
            for c in range(2):
                tell(entered, {"tp": (z - dz) * 2 + c})

    def hand_over(w, k, of):
        return pltpu.make_async_remote_copy(
            src_ref=lowered.at[w, token_rows(k, of)],
            dst_ref=lowered.at[w, token_rows(k, of)],
            send_sem=half_send,
            recv_sem=half_recv.at[w, k],
            device_id=partner,
            device_id_type=MESH,
        )

    def project(w, k):
        low = jnp.dot(tokens[w, k], basis[w], preferred_element_type=F32)
        high = low.astype(BF16)
        rest = (low - high.astype(F32)).astype(BF16)
        rank = low.shape[1]
        lowered[w, token_rows(k), pl.ds(0, rank)] = high
        lowered[w, token_rows(k), pl.ds(rank, rank)] = rest
        op = hand_over(w, k, core)
        op.start()

    def contract(w, of):
        half = pl.ds(pl.multiple_of(of * share, share), share)
        return lax.dot_general(
            lowered[w, half], cotangents[w, half], OVER_ROWS, preferred_element_type=F32
        )

    def finish(w):
        both = contract(w, core)
        for k in range(chunks):
            hand_over(w, k, 1 - core).wait_recv()
        both += contract(w, 1 - core)
        rank = both.shape[0] // 2
        total = both[:rank] + both[rank:]
        partial[w] = total.reshape(FS, rank // FS, total.shape[1])

    def next_round(k):
        pl.semaphore_wait(round_sem.at[k], len(near))
        if k < 2:
            greet(round_sem.at[k + 1])

    loads[2].wait()
    first = 3
    for w in range(2):
        if w == 1:
            loads[first].wait()
            loads[first + 1].wait()
            first += 2
        for k in range(chunks):
            loads[first + k].wait()
            project(w, k)
            if w == 1 and k == 0:
                next_round(0)
                finish(0)
            if w == 1 and k == 2:
                next_round(1)
        first += chunks
    loads[first].wait()
    finish(1)
    first += 1
    partial_out[...] = jnp.concatenate([partial[0], partial[1]], axis=1).astype(BF16)
    next_round(2)

    for j in range(1, FS):
        target = lax.rem(fs_me + j, FS)
        op = pltpu.make_async_remote_copy(
            src_ref=partial_out.at[target],
            dst_ref=partial_in.at[j],
            send_sem=part_send,
            recv_sem=part_recv,
            device_id={"fs": target},
            device_id_type=MESH,
        )
        op.start()

    for w in range(2):
        first_relay(w)
    for w in range(2):
        second_own(w, 1)

    grams = []
    for w in range(2):
        gram = lax.dot_general(basis[w], basis[w], OVER_ROWS, preferred_element_type=F32)
        grams.append(gram)

    for load in loads[first:]:
        load.wait()
    def together(refs, sems):
        return pltpu.make_async_remote_copy(
            src_ref=refs,
            dst_ref=refs,
            send_sem=sems[0],
            recv_sem=sems[1],
            device_id=partner,
            device_id_type=MESH,
        )

    others = pl.ds(1, FS - 1)
    parts = together(partial_in.at[others], (part_send, part_recv))
    parts.wait_recv()
    incoming = jnp.sum(partial_in[pl.ds(1, FS - 1)].astype(F32), axis=0)
    moments = (
        (query_first_new, query_second_new),
        (output_first_new, output_second_new),
    )
    ratios = []
    for w in range(2):
        own = partial[w, fs_me]
        rank_rows = own.shape[0]
        low = own + incoming[w * rank_rows : (w + 1) * rank_rows]
        first_new = FIRST_DECAY * moment[2 * w] + (1.0 - FIRST_DECAY) * low
        second_new = SECOND_DECAY * moment[2 * w + 1] + (1.0 - SECOND_DECAY) * low * low
        moments[w][0][...] = first_new
        moments[w][1][...] = second_new
        ratios.append(first_new / jnp.sqrt(second_new + SECOND_FLOOR))
    ratio_all[fs_me] = jnp.concatenate(ratios, axis=0).astype(BF16)

    for j in range(1, FS):
        op = pltpu.make_async_remote_copy(
            src_ref=ratio_all.at[fs_me],
            dst_ref=ratio_all.at[fs_me],
            send_sem=ratio_send,
            recv_sem=ratio_recv,
            device_id={"fs": lax.rem(fs_me + j, FS)},
            device_id_type=MESH,
        )
        op.start()

    for k in (2, 3):
        for w in range(2):
            second_own(w, k)
    for w in range(2):
        second_relay(w, 0)

    shared = together(ratio_all.at[others], (ratio_send, ratio_recv))
    shared.wait_recv()
    every = ratio_all[...].astype(F32)
    rank_rows = every.shape[1] // 2
    full_ratio = []
    squares = []
    for w in range(2):
        ratio = every[:, w * rank_rows : (w + 1) * rank_rows, :].reshape(-1, every.shape[2])
        ratio_low = ratio.astype(BF16)
        full_ratio.append(ratio_low)
        high = grams[w].astype(BF16)
        rest = (grams[w] - high.astype(F32)).astype(BF16)
        spread = jnp.dot(high, ratio_low, preferred_element_type=F32)
        spread += jnp.dot(rest, ratio_low, preferred_element_type=F32)
        squares.append(jnp.sum(ratio * spread))
    lane = lax.broadcasted_iota(jnp.int32, square_out.shape, 1)
    shares = jnp.where(lane < square_out.shape[1] // 2, squares[0], squares[1])
    square_out[...] = shares
    square_in[0] = shares

    @pl.when(z < heights - 1)
    def _():
        pl.semaphore_wait(entered, 2 * (heights - 1 - z))

    for j in range(1, tp):
        op = pltpu.make_async_remote_copy(
            src_ref=square_out,
            dst_ref=square_in.at[j],
            send_sem=square_send,
            recv_sem=square_recv,
            device_id={"tp": lax.rem(tp_me + j, tp)},
            device_id_type=MESH,
        )
        op.start()

    @pl.loop(0, FS // 2)
    def _(k):
        for w in range(2):
            pair = pl.ds(pl.multiple_of(2 * rows * k, 2 * rows), 2 * rows)
            product = jnp.dot(basis[w, pair], full_ratio[w], preferred_element_type=F32)
            product = product.reshape(2, rows, product.shape[1])
            update[w, pl.ds(2 * k, 2)] = product.astype(BF16)

    for k in (1, 2):
        for w in range(2):
            second_relay(w, k)
    own_rows = pl.ds(pl.multiple_of(fs_me * rows, rows), rows)
    for w in range(2):
        own_update[w] = jnp.dot(
            basis[w, own_rows], full_ratio[w], preferred_element_type=F32
        )
    for w in range(2):
        second_relay(w, 3)

    totals = together(square_in.at[pl.ds(1, tp - 1)], (square_send, square_recv))
    totals.wait_recv()
    entries = basis.shape[1] * full_ratio[0].shape[1] * tp
    factors = lax.rsqrt(jnp.sum(square_in[...], axis=0) / entries + SCALE_FLOOR)
    scales[...] = factors

    own_share = lowered.at[:, pl.ds(0, share)]
    together(own_share, (half_send, half_recv.at[0, 0])).wait_send()
    parts.wait_send()
    shared.wait_send()
    totals.wait_send()
    for k in range(4):
        for w in range(2):
            second_last(w, k)
    for w in range(2):
        together(gathered.at[w, others], (block_send.at[w], block_recv.at[w, 0])).wait_send()


def store_kernel(
    gathered,
    update,
    own_update,
    master,
    scales,
    query_first,
    query_second,
    output_first,
    output_second,
    query_first_new,
    query_second_new,
    query_step,
    query_new,
    query_copy,
    output_first_new,
    output_second_new,
    output_step,
    output_new,
    output_copy,
    copies,
    steps,
    news,
    copy_sem,
    other_sem,
):
    moments = ((query_first, query_second), (output_first, output_second))
    outputs = (
        (query_first_new, query_second_new, query_step, query_new, query_copy),
        (output_first_new, output_second_new, output_step, output_new, output_copy),
    )
    half = scales.shape[1] // 2
    scale = [scales[0:1, 0:1], scales[0:1, half : half + 1]]
    rate = [(LEARN_RATE * scale[w]).astype(BF16) for w in range(2)]

    copying = []

    def put(w, number, source):
        copying.append(
            pltpu.make_async_copy(source, outputs[w][number], other_sem.at[w, number])
        )
        copying[-1].start()

    for owner in range(FS):
        for w in range(2):
            copies[w, owner] = gathered[w, owner] - rate[w] * update[w, owner]
            pltpu.make_async_copy(
                copies.at[w, owner], outputs[w][4].at[owner], copy_sem.at[w]
            ).start()

    for w in range(2):
        put(w, 0, moments[w][0])
        put(w, 1, moments[w][1])
        step = own_update[w] * scale[w]
        steps[w] = step
        put(w, 2, steps.at[w])
        news[w] = master[w] - LEARN_RATE * step
        put(w, 3, news.at[w])

    for w in range(2):
        pltpu.make_async_copy(copies.at[w], outputs[w][4], copy_sem.at[w]).wait()
    for copy in copying:
        copy.wait()


def body(
    normed,
    query_cotangent,
    attended,
    output_cotangent,
    query_basis,
    output_basis,
    query_master,
    output_master,
    query_first,
    query_second,
    output_first,
    output_second,
):
    operands = (
        normed,
        query_cotangent,
        attended,
        output_cotangent,
        query_basis,
        output_basis,
        query_master,
        output_master,
        query_first,
        query_second,
        output_first,
        output_second,
    )
    tp = lax.axis_size("tp")
    token_rows, width = normed.shape
    rank = query_basis.shape[1]
    rows, columns = query_master.shape
    rank_rows = query_first.shape[0]
    blocks, block, small = (2, FS, rows, columns), (2, rows, columns), (rank_rows, columns)
    pieces = token_rows // 2 // CHUNK
    exchanged = pl.pallas_call(
        lambda *refs: kernel(tp, *refs),
        out_shape=[
            pltpu.VMEM(blocks, BF16),
            pltpu.VMEM(blocks, BF16),
            pltpu.VMEM(block, F32),
            pltpu.VMEM(block, F32),
            pltpu.VMEM((1, 128), F32),
            pltpu.VMEM(small, F32),
            pltpu.VMEM(small, F32),
            pltpu.VMEM(small, F32),
            pltpu.VMEM(small, F32),
        ],
        in_specs=[pl.BlockSpec(memory_space=pltpu.HBM)] * 12,
        out_specs=[pl.BlockSpec(memory_space=pltpu.VMEM)] * 9,
        scratch_shapes=[
            pltpu.VMEM((2, pieces, CHUNK, width), BF16),
            pltpu.VMEM((2, width, rank), BF16),
            pltpu.VMEM((2, token_rows, columns), BF16),
            pltpu.VMEM((4, rank_rows, columns), F32),
            pltpu.VMEM((2, token_rows, 2 * rank), BF16),
            pltpu.VMEM((2, FS, rank_rows, columns), F32),
            pltpu.VMEM((FS, 2 * rank_rows, columns), BF16),
            pltpu.VMEM((FS, 2 * rank_rows, columns), BF16),
            pltpu.VMEM((FS, 2 * rank_rows, columns), BF16),
            pltpu.VMEM((1, 128), F32),
            pltpu.VMEM((tp, 1, 128), F32),
            pltpu.SemaphoreType.DMA((2,)),
            pltpu.SemaphoreType.DMA((2, 20)),
            pltpu.SemaphoreType.DMA,
            pltpu.SemaphoreType.DMA,
            pltpu.SemaphoreType.DMA,
            pltpu.SemaphoreType.DMA,
            pltpu.SemaphoreType.DMA,
            pltpu.SemaphoreType.DMA,
            pltpu.SemaphoreType.DMA,
            pltpu.SemaphoreType.DMA((2, pieces)),
            pltpu.SemaphoreType.DMA((10 + 2 * pieces,)),
            pltpu.SemaphoreType.REGULAR((3,)),
            pltpu.SemaphoreType.REGULAR,
        ],
        compiler_params=pltpu.CompilerParams(
            collective_id=0, has_side_effects=True, vmem_limit_bytes=28 * 1024 * 1024
        ),
        name="exchange",
    )(*(pltpu.with_memory_space_constraint(operand, pltpu.HBM) for operand in operands))
    per_weight = (
        jax.ShapeDtypeStruct(small, F32),
        jax.ShapeDtypeStruct(small, F32),
        jax.ShapeDtypeStruct((rows, columns), F32),
        jax.ShapeDtypeStruct((rows, columns), F32),
        jax.ShapeDtypeStruct((FS, rows, columns), BF16),
    )
    results = pl.pallas_call(
        store_kernel,
        out_shape=per_weight * 2,
        in_specs=[pl.BlockSpec(memory_space=pltpu.VMEM)] * 9,
        out_specs=[pl.BlockSpec(memory_space=pl.ANY)] * 10,
        scratch_shapes=[
            pltpu.VMEM(blocks, BF16),
            pltpu.VMEM(block, F32),
            pltpu.VMEM(block, F32),
            pltpu.SemaphoreType.DMA((2,)),
            pltpu.SemaphoreType.DMA((2, 4)),
        ],
        compiler_params=pltpu.CompilerParams(vmem_limit_bytes=16 * 1024 * 1024),
        name="store",
    )(*exchanged)
    return tuple(r.reshape(-1, columns) for r in results)


def solution(mesh):
    in_specs = (
        P("fs", None),
        P("fs", "tp"),
        P("fs", "tp"),
        P("fs", None),
        P(),
        P(),
        P("fs", "tp"),
        P("fs", "tp"),
        P("fs", "tp"),
        P("fs", "tp"),
        P("fs", "tp"),
        P("fs", "tp"),
    )
    out_specs = (
        P("fs", "tp"),
        P("fs", "tp"),
        P("fs", "tp"),
        P("fs", "tp"),
        P(None, "tp"),
        P("fs", "tp"),
        P("fs", "tp"),
        P("fs", "tp"),
        P("fs", "tp"),
        P(None, "tp"),
    )
    return jax.shard_map(body, mesh=mesh, in_specs=in_specs, out_specs=out_specs, check_vma=False)
```

```python
import jax
import jax.numpy as jnp
from jax import lax
from jax.experimental import pallas as pl
from jax.experimental.pallas import tpu as pltpu
from jax.sharding import PartitionSpec as P

FIRST_DECAY = 0.7
SECOND_DECAY = 0.8
SECOND_FLOOR = 0.05
SCALE_FLOOR = 0.01
LEARN_RATE = 0.05
OVER_ROWS = (((0,), (0,)), ((), ()))
MESH = pl.DeviceIdType.MESH
F32, BF16 = jnp.float32, jnp.bfloat16

SIDE = 4
FS = SIDE * SIDE
CHUNK = 256
UPPER = 112
STEPS = (0, -1, 1, 2)


def hops(offset, size):
    return min(offset, size - offset)


OTHERS = sorted(
    ((dy, dx) for dy in range(SIDE) for dx in range(SIDE) if dy or dx),
    key=lambda o: -hops(o[0], SIDE) - hops(o[1], SIDE),
)


def kernel(
    tp,
    normed,
    query_cotangent,
    attended,
    output_cotangent,
    query_basis,
    output_basis,
    query_master,
    output_master,
    query_first,
    query_second,
    output_first,
    output_second,
    gathered,
    update,
    own_update,
    master,
    scales,
    query_first_new,
    query_second_new,
    output_first_new,
    output_second_new,
    tokens,
    basis,
    cotangents,
    moment,
    lowered,
    partial,
    partial_out,
    partial_in,
    ratio_all,
    square_out,
    square_in,
    block_send,
    block_recv,
    part_send,
    part_recv,
    ratio_send,
    ratio_recv,
    square_send,
    square_recv,
    half_send,
    half_recv,
    local_sem,
    round_sem,
    entered,
):
    fs_me = lax.axis_index("fs")
    tp_me = lax.axis_index("tp")
    y, x = fs_me // SIDE, fs_me % SIDE
    z, core = tp_me // 2, tp_me % 2
    heights = tp // 2

    def at(dy, dx):
        return ((y + dy + SIDE) % SIDE) * SIDE + (x + dx + SIDE) % SIDE

    def up(dz):
        return ((z + dz + heights) % heights) * 2 + core

    near = [{"fs": at(0, 1)}, {"fs": at(0, -1)}, {"fs": at(1, 0)}, {"fs": at(-1, 0)}]
    partner = {"tp": z * 2 + (1 - core)}

    def tell(sem, device):
        pl.semaphore_signal(sem, inc=1, device_id=device, device_id_type=MESH)

    def greet(sem):
        for device in near:
            tell(sem, device)

    sources = (normed, output_cotangent)
    share = normed.shape[0] // 2
    chunks = share // CHUNK

    def token_rows(chunk, of=core):
        return pl.ds(pl.multiple_of(of * share + chunk * CHUNK, CHUNK), CHUNK)

    pieces = [
        (query_master, master.at[0]),
        (output_master, master.at[1]),
        (query_basis, basis.at[0]),
    ]
    for w in range(2):
        for k in range(chunks):
            pieces.append((sources[w].at[token_rows(k)], tokens.at[w, k]))
        if w == 0:
            pieces.append((query_cotangent, cotangents.at[0]))
            pieces.append((output_basis, basis.at[1]))
        else:
            pieces.append((attended, cotangents.at[1]))
    pieces += [
        (query_first, moment.at[0]),
        (query_second, moment.at[1]),
        (output_first, moment.at[2]),
        (output_second, moment.at[3]),
    ]
    loads = []
    for k, (src, dst) in enumerate(pieces):
        loads.append(pltpu.make_async_copy(src, dst, local_sem.at[k]))
    for load in loads[:2]:
        load.start()

    barrier = pltpu.get_barrier_semaphore()
    greet(barrier)
    tell(barrier, partner)
    for dz in range(1, heights):

        @pl.when(z + dz < heights)
        def _():
            for c in range(2):
                tell(barrier, {"tp": (z + dz) * 2 + c})

    for load in loads[2:]:
        load.start()

    for w in range(2):
        loads[w].wait()
        gathered[w, fs_me] = master[w].astype(BF16)

    rows = gathered.shape[2]
    upper, lower, full = pl.ds(0, UPPER), pl.ds(UPPER, rows - UPPER), pl.ds(0, rows)

    def place(w, da, db):
        return at(db, da) if w == 0 else at(da, db)

    def send(w, number, along_a, sign, block, rows):
        device = place(w, sign, 0) if along_a else place(w, 0, sign)
        piece = gathered.at[w, place(w, *block), rows]
        op = pltpu.make_async_remote_copy(
            src_ref=piece,
            dst_ref=piece,
            send_sem=block_send.at[w],
            recv_sem=block_recv.at[w, number],
            device_id={"fs": device},
            device_id_type=MESH,
        )
        op.start()

    def arrived(w, number, block, rows):
        piece = gathered.at[w, place(w, *block), rows]
        pltpu.make_async_remote_copy(
            src_ref=piece,
            dst_ref=piece,
            send_sem=block_send.at[w],
            recv_sem=block_recv.at[w, number],
            device_id={"fs": at(0, 1)},
            device_id_type=MESH,
        ).wait_recv()

    def first_own(w):
        send(w, 0, True, 1, (0, 0), full)
        send(w, 1, True, -1, (0, 0), full)

    def first_relay(w):
        arrived(w, 0, (-1, 0), full)
        send(w, 2, True, 1, (-1, 0), upper)
        arrived(w, 1, (1, 0), full)
        send(w, 3, True, -1, (1, 0), lower)

    def second_own(w, k):
        if k == 3:
            arrived(w, 2, (2, 0), upper)
            arrived(w, 3, (2, 0), lower)
        send(w, 4 + 2 * k, False, 1, (STEPS[k], 0), full)
        send(w, 5 + 2 * k, False, -1, (STEPS[k], 0), full)

    def second_relay(w, k):
        arrived(w, 4 + 2 * k, (STEPS[k], -1), full)
        send(w, 12 + 2 * k, False, 1, (STEPS[k], -1), upper)
        arrived(w, 5 + 2 * k, (STEPS[k], 1), full)
        send(w, 13 + 2 * k, False, -1, (STEPS[k], 1), lower)

    def second_last(w, k):
        arrived(w, 12 + 2 * k, (STEPS[k], 2), upper)
        arrived(w, 13 + 2 * k, (STEPS[k], 2), lower)

    pl.semaphore_wait(barrier, len(near) + 1 + 2 * z)
    for w in range(2):
        first_own(w)
    for w in range(2):
        second_own(w, 0)
    greet(round_sem.at[0])
    for dz in range(1, heights):

        @pl.when(z - dz >= 0)
        def _():
            for c in range(2):
                tell(entered, {"tp": (z - dz) * 2 + c})

    def hand_over(w, k, of):
        return pltpu.make_async_remote_copy(
            src_ref=lowered.at[w, token_rows(k, of)],
            dst_ref=lowered.at[w, token_rows(k, of)],
            send_sem=half_send,
            recv_sem=half_recv.at[w, k],
            device_id=partner,
            device_id_type=MESH,
        )

    def project(w, k):
        low = jnp.dot(tokens[w, k], basis[w], preferred_element_type=F32)
        high = low.astype(BF16)
        rest = (low - high.astype(F32)).astype(BF16)
        rank = low.shape[1]
        lowered[w, token_rows(k), pl.ds(0, rank)] = high
        lowered[w, token_rows(k), pl.ds(rank, rank)] = rest
        op = hand_over(w, k, core)
        op.start()

    def contract(w, of):
        half = pl.ds(pl.multiple_of(of * share, share), share)
        return lax.dot_general(
            lowered[w, half], cotangents[w, half], OVER_ROWS, preferred_element_type=F32
        )

    def finish(w):
        both = contract(w, core)
        for k in range(chunks):
            hand_over(w, k, 1 - core).wait_recv()
        both += contract(w, 1 - core)
        rank = both.shape[0] // 2
        total = both[:rank] + both[rank:]
        partial[w] = total.reshape(FS, rank // FS, total.shape[1])

    def next_round(k):
        pl.semaphore_wait(round_sem.at[k], len(near))
        if k < 2:
            greet(round_sem.at[k + 1])

    loads[2].wait()
    first = 3
    for w in range(2):
        if w == 1:
            loads[first].wait()
            loads[first + 1].wait()
            first += 2
        for k in range(chunks):
            loads[first + k].wait()
            project(w, k)
            if w == 1 and k == 0:
                next_round(0)
                finish(0)
            if w == 1 and k == chunks - 1:
                next_round(1)
        first += chunks
    loads[first].wait()
    finish(1)
    first += 1
    partial_out[...] = jnp.concatenate([partial[0], partial[1]], axis=1).astype(BF16)
    next_round(2)

    for dy, dx in OTHERS:
        target = at(dy, dx)
        op = pltpu.make_async_remote_copy(
            src_ref=partial_out.at[target],
            dst_ref=partial_in.at[dy * SIDE + dx],
            send_sem=part_send,
            recv_sem=part_recv,
            device_id={"fs": target},
            device_id_type=MESH,
        )
        op.start()

    for w in range(2):
        first_relay(w)
    for w in range(2):
        second_own(w, 1)

    grams = []
    for w in range(2):
        gram = lax.dot_general(basis[w], basis[w], OVER_ROWS, preferred_element_type=F32)
        grams.append(gram)

    for load in loads[first:]:
        load.wait()
    def together(refs, sems):
        return pltpu.make_async_remote_copy(
            src_ref=refs,
            dst_ref=refs,
            send_sem=sems[0],
            recv_sem=sems[1],
            device_id=partner,
            device_id_type=MESH,
        )

    others = pl.ds(1, FS - 1)
    parts = together(partial_in.at[others], (part_send, part_recv))
    parts.wait_recv()
    incoming = jnp.sum(partial_in[pl.ds(1, FS - 1)].astype(F32), axis=0)
    moments = (
        (query_first_new, query_second_new),
        (output_first_new, output_second_new),
    )
    ratios = []
    for w in range(2):
        own = partial[w, fs_me]
        rank_rows = own.shape[0]
        low = own + incoming[w * rank_rows : (w + 1) * rank_rows]
        first_new = FIRST_DECAY * moment[2 * w] + (1.0 - FIRST_DECAY) * low
        second_new = SECOND_DECAY * moment[2 * w + 1] + (1.0 - SECOND_DECAY) * low * low
        moments[w][0][...] = first_new
        moments[w][1][...] = second_new
        ratios.append(first_new / jnp.sqrt(second_new + SECOND_FLOOR))
    ratio_all[fs_me] = jnp.concatenate(ratios, axis=0).astype(BF16)

    for dy, dx in OTHERS:
        op = pltpu.make_async_remote_copy(
            src_ref=ratio_all.at[fs_me],
            dst_ref=ratio_all.at[fs_me],
            send_sem=ratio_send,
            recv_sem=ratio_recv,
            device_id={"fs": at(dy, dx)},
            device_id_type=MESH,
        )
        op.start()

    for k in (2, 3):
        for w in range(2):
            second_own(w, k)
    for w in range(2):
        second_relay(w, 0)

    shared = together(ratio_all.at[others], (ratio_send, ratio_recv))
    shared.wait_recv()
    every = ratio_all[...].astype(F32)
    rank_rows = every.shape[1] // 2
    full_ratio = []
    squares = []
    for w in range(2):
        ratio = every[:, w * rank_rows : (w + 1) * rank_rows, :].reshape(-1, every.shape[2])
        ratio_low = ratio.astype(BF16)
        full_ratio.append(ratio_low)
        high = grams[w].astype(BF16)
        rest = (grams[w] - high.astype(F32)).astype(BF16)
        spread = jnp.dot(high, ratio_low, preferred_element_type=F32)
        spread += jnp.dot(rest, ratio_low, preferred_element_type=F32)
        squares.append(jnp.sum(ratio * spread))
    lane = lax.broadcasted_iota(jnp.int32, square_out.shape, 1)
    shares = jnp.where(lane < square_out.shape[1] // 2, squares[0], squares[1])
    square_out[...] = shares
    square_in[0] = shares

    @pl.when(z < heights - 1)
    def _():
        pl.semaphore_wait(entered, 2 * (heights - 1 - z))

    peers = sorted(
        ((dz, c) for dz in range(heights) for c in range(2) if dz or c),
        key=lambda o: -hops(o[0], heights),
    )
    for dz, c in peers:
        op = pltpu.make_async_remote_copy(
            src_ref=square_out,
            dst_ref=square_in.at[2 * dz + c],
            send_sem=square_send,
            recv_sem=square_recv,
            device_id={"tp": ((z + dz) % heights) * 2 + (core + c) % 2},
            device_id_type=MESH,
        )
        op.start()

    @pl.loop(0, FS // 2)
    def _(k):
        for w in range(2):
            pair = pl.ds(pl.multiple_of(2 * rows * k, 2 * rows), 2 * rows)
            product = jnp.dot(basis[w, pair], full_ratio[w], preferred_element_type=F32)
            product = product.reshape(2, rows, product.shape[1])
            update[w, pl.ds(2 * k, 2)] = product.astype(BF16)

    for k in (1, 2):
        for w in range(2):
            second_relay(w, k)
    own_rows = pl.ds(pl.multiple_of(fs_me * rows, rows), rows)
    for w in range(2):
        own_update[w] = jnp.dot(
            basis[w, own_rows], full_ratio[w], preferred_element_type=F32
        )
    for w in range(2):
        second_relay(w, 3)

    totals = together(square_in.at[pl.ds(1, tp - 1)], (square_send, square_recv))
    totals.wait_recv()
    entries = basis.shape[1] * full_ratio[0].shape[1] * tp
    factors = lax.rsqrt(jnp.sum(square_in[...], axis=0) / entries + SCALE_FLOOR)
    scales[...] = factors

    own_share = lowered.at[:, pl.ds(0, share)]
    together(own_share, (half_send, half_recv.at[0, 0])).wait_send()
    parts.wait_send()
    shared.wait_send()
    totals.wait_send()
    for k in range(4):
        for w in range(2):
            second_last(w, k)
    for w in range(2):
        together(gathered.at[w, others], (block_send.at[w], block_recv.at[w, 0])).wait_send()


def store_kernel(
    gathered,
    update,
    own_update,
    master,
    scales,
    query_first,
    query_second,
    output_first,
    output_second,
    query_first_new,
    query_second_new,
    query_step,
    query_new,
    query_copy,
    output_first_new,
    output_second_new,
    output_step,
    output_new,
    output_copy,
    copies,
    steps,
    news,
    copy_sem,
    other_sem,
):
    moments = ((query_first, query_second), (output_first, output_second))
    outputs = (
        (query_first_new, query_second_new, query_step, query_new, query_copy),
        (output_first_new, output_second_new, output_step, output_new, output_copy),
    )
    half = scales.shape[1] // 2
    scale = [scales[0:1, 0:1], scales[0:1, half : half + 1]]
    rate = [(LEARN_RATE * scale[w]).astype(BF16) for w in range(2)]

    copying = []

    def put(w, number, source):
        copying.append(
            pltpu.make_async_copy(source, outputs[w][number], other_sem.at[w, number])
        )
        copying[-1].start()

    for owner in range(FS):
        for w in range(2):
            copies[w, owner] = gathered[w, owner] - rate[w] * update[w, owner]
            pltpu.make_async_copy(
                copies.at[w, owner], outputs[w][4].at[owner], copy_sem.at[w]
            ).start()

    for w in range(2):
        put(w, 0, moments[w][0])
        put(w, 1, moments[w][1])
        step = own_update[w] * scale[w]
        steps[w] = step
        put(w, 2, steps.at[w])
        news[w] = master[w] - LEARN_RATE * step
        put(w, 3, news.at[w])

    for w in range(2):
        pltpu.make_async_copy(copies.at[w], outputs[w][4], copy_sem.at[w]).wait()
    for copy in copying:
        copy.wait()


def body(
    normed,
    query_cotangent,
    attended,
    output_cotangent,
    query_basis,
    output_basis,
    query_master,
    output_master,
    query_first,
    query_second,
    output_first,
    output_second,
):
    operands = (
        normed,
        query_cotangent,
        attended,
        output_cotangent,
        query_basis,
        output_basis,
        query_master,
        output_master,
        query_first,
        query_second,
        output_first,
        output_second,
    )
    tp = lax.axis_size("tp")
    token_rows, width = normed.shape
    rank = query_basis.shape[1]
    rows, columns = query_master.shape
    rank_rows = query_first.shape[0]
    blocks, block, small = (2, FS, rows, columns), (2, rows, columns), (rank_rows, columns)
    pieces = token_rows // 2 // CHUNK
    exchanged = pl.pallas_call(
        lambda *refs: kernel(tp, *refs),
        out_shape=[
            pltpu.VMEM(blocks, BF16),
            pltpu.VMEM(blocks, BF16),
            pltpu.VMEM(block, F32),
            pltpu.VMEM(block, F32),
            pltpu.VMEM((1, 128), F32),
            pltpu.VMEM(small, F32),
            pltpu.VMEM(small, F32),
            pltpu.VMEM(small, F32),
            pltpu.VMEM(small, F32),
        ],
        in_specs=[pl.BlockSpec(memory_space=pltpu.HBM)] * 12,
        out_specs=[pl.BlockSpec(memory_space=pltpu.VMEM)] * 9,
        scratch_shapes=[
            pltpu.VMEM((2, pieces, CHUNK, width), BF16),
            pltpu.VMEM((2, width, rank), BF16),
            pltpu.VMEM((2, token_rows, columns), BF16),
            pltpu.VMEM((4, rank_rows, columns), F32),
            pltpu.VMEM((2, token_rows, 2 * rank), BF16),
            pltpu.VMEM((2, FS, rank_rows, columns), F32),
            pltpu.VMEM((FS, 2 * rank_rows, columns), BF16),
            pltpu.VMEM((FS, 2 * rank_rows, columns), BF16),
            pltpu.VMEM((FS, 2 * rank_rows, columns), BF16),
            pltpu.VMEM((1, 128), F32),
            pltpu.VMEM((tp, 1, 128), F32),
            pltpu.SemaphoreType.DMA((2,)),
            pltpu.SemaphoreType.DMA((2, 20)),
            pltpu.SemaphoreType.DMA,
            pltpu.SemaphoreType.DMA,
            pltpu.SemaphoreType.DMA,
            pltpu.SemaphoreType.DMA,
            pltpu.SemaphoreType.DMA,
            pltpu.SemaphoreType.DMA,
            pltpu.SemaphoreType.DMA,
            pltpu.SemaphoreType.DMA((2, pieces)),
            pltpu.SemaphoreType.DMA((10 + 2 * pieces,)),
            pltpu.SemaphoreType.REGULAR((3,)),
            pltpu.SemaphoreType.REGULAR,
        ],
        compiler_params=pltpu.CompilerParams(
            collective_id=0, has_side_effects=True, vmem_limit_bytes=28 * 1024 * 1024
        ),
        name="exchange",
    )(*(pltpu.with_memory_space_constraint(operand, pltpu.HBM) for operand in operands))
    per_weight = (
        jax.ShapeDtypeStruct(small, F32),
        jax.ShapeDtypeStruct(small, F32),
        jax.ShapeDtypeStruct((rows, columns), F32),
        jax.ShapeDtypeStruct((rows, columns), F32),
        jax.ShapeDtypeStruct((FS, rows, columns), BF16),
    )
    results = pl.pallas_call(
        store_kernel,
        out_shape=per_weight * 2,
        in_specs=[pl.BlockSpec(memory_space=pltpu.VMEM)] * 9,
        out_specs=[pl.BlockSpec(memory_space=pl.ANY)] * 10,
        scratch_shapes=[
            pltpu.VMEM(blocks, BF16),
            pltpu.VMEM(block, F32),
            pltpu.VMEM(block, F32),
            pltpu.SemaphoreType.DMA((2,)),
            pltpu.SemaphoreType.DMA((2, 4)),
        ],
        compiler_params=pltpu.CompilerParams(vmem_limit_bytes=16 * 1024 * 1024),
        name="store",
    )(*exchanged)
    return tuple(r.reshape(-1, columns) for r in results)


def solution(mesh):
    in_specs = (
        P("fs", None),
        P("fs", "tp"),
        P("fs", "tp"),
        P("fs", None),
        P(),
        P(),
        P("fs", "tp"),
        P("fs", "tp"),
        P("fs", "tp"),
        P("fs", "tp"),
        P("fs", "tp"),
        P("fs", "tp"),
    )
    out_specs = (
        P("fs", "tp"),
        P("fs", "tp"),
        P("fs", "tp"),
        P("fs", "tp"),
        P(None, "tp"),
        P("fs", "tp"),
        P("fs", "tp"),
        P("fs", "tp"),
        P("fs", "tp"),
        P(None, "tp"),
    )
    return jax.shard_map(body, mesh=mesh, in_specs=in_specs, out_specs=out_specs, check_vma=False)
```
